256 devices in a mesh: grp: 2 (over z), sp: 16 (over y, core), tp: 8 (over x).
Axes of the slice: x: 8, y: 8, z: 2, core: 2. Of those that a mesh axis runs over, the one named last changes fastest.
The devices are a block of a 8x8x16 slice.
Arguments:
- residual: bfloat16 [3072, 8, 2048], P(('sp', 'tp'), 'grp'), parts along dimension 1, may hold values from -6 to 6
- query: bfloat16 [3072, 8, 1536], P('sp', 'grp', 'tp'), parts along dimension 1, may hold values from -64 to 64
- latent: bfloat16 [3072, 8, 512], P('sp', 'grp'), parts along dimension 1, may hold values from -6 to 6
- rope_key: bfloat16 [3072, 8, 64], P('sp', 'grp'), parts along dimension 1, may hold values from -8 to 8
- latent_gain: float32 [512], replicated, may hold values from 0.1 to 1.9
- key_up: bfloat16 [512, 1024], P(None, 'tp'), may hold values from -0.25 to 0.25
- value_up: bfloat16 [512, 1024], P(None, 'tp'), may hold values from -0.25 to 0.25
- out_weight: bfloat16 [1024, 2048], P('tp'), may hold values from -0.375 to 0.375
- norm_gain: float32 [2048], replicated, may hold values from 0.1 to 1.9
- group_prob: float32 [3072, 8], P(('sp', 'tp'), 'grp'), parts along dimension 1, may hold values from 0.25 to 1
- pair_logits: float32 [3072, 8, 2], P(('sp', 'tp'), 'grp'), parts along dimension 1, may hold values from -8 to 8
- routes: int32 [3072, 8, 2], P(('sp', 'tp'), 'grp'), parts along dimension 1, may hold values from 0 to 127, all different within a row; in each aligned block of 96 rows (0 to 95, 96 to 191, ..., all dimensions but the last counted through in order) at most 2 rows name the same one
- w_gate: bfloat16 [128, 2048, 768], P(('sp', 'tp')), may hold values from -0.125 to 0.125
- w_up: bfloat16 [128, 2048, 768], P(('sp', 'tp')), may hold values from -0.125 to 0.125
- w_down: bfloat16 [128, 768, 2048], P(('sp', 'tp')), may hold values from -0.4375 to 0.4375
Outputs:
- layer_out: bfloat16 [3072, 8, 2048], P(('sp', 'tp'), 'grp'), parts along dimension 1
The draws below stay inside these ranges and needn't reach their ends.
There are 2 independent parts, one for each index of `grp`. The reference program is written for one: setup_inputs(seed, part) draws one part's arguments, and reference() takes and returns one part's arrays. A program takes and returns all parts, laid end to end along the dimension named above; an argument that names none is the same for every part. Nothing has to cross between parts.
Inputs may be any that keep to these rules, and one draw needn't show every extreme that they name: `routes`: A token's 2 experts differ. Among the tokens of one device (aligned blocks of 96 rows in position-then-sequence order), no expert is named more than 2 times, a bound that some block reaches.
All inputs are finite; a program needn't handle non-finite values.
Results may differ from the reference program's by a relative error of at most 0.013.
Values may be sent and summed in bfloat16 or wider, within the bound.
A program may use at most 128 MiB of HBM per device.

```python
import math
import jax
import jax.numpy as jnp
import numpy as np
from jax import lax

D = 2048
HEADS = 8
NOPE = 128
ROPE = 64
VDIM = 128
QK = 192
LATENT = 512
FF = 768
TOPK = 2
SEQS = 4
LEN = 3072
ROWS_DEV = 96
EXPERTS = 128
CAP = 2


def draw_rope_key(key, part):
    shape_all = (LEN, SEQS, ROPE)
    drawn = jnp.clip(jax.random.normal(jax.random.fold_in(key, 2), shape_all, jnp.float32), -6.0, 6.0)
    return drawn.astype(jnp.bfloat16)


def draw_query(key, part):
    shape_all = (LEN, SEQS, HEADS * QK)
    drawn = jnp.clip(2.5 * jax.random.normal(jax.random.fold_in(key, 1), shape_all, jnp.float32), -15.0, 15.0)
    return drawn.astype(jnp.bfloat16)


def block_levels(rng, dims, pieces, least, top_value):
    gain, own = 1.0, jax.random.fold_in(rng, 6)
    for position, blocks in pieces:
        steps = jnp.exp(jax.random.uniform(jax.random.fold_in(own, position), (blocks,), jnp.float32, least / len(pieces), top_value / len(pieces)))
        gain = gain * jnp.repeat(steps, dims[position] // blocks).reshape([-1 if axis == position else 1 for axis in range(len(dims))])
    return gain


def assign_block(stream_key, own, number, rows, count, top, bound, skew):
    order = jax.random.permutation(stream_key, count)
    packed, common = load_shares(count, rows * top, bound, skew, True), load_shares(count, rows * top, bound, skew, False)
    places = jnp.arange(count)

    def named(lengths, rotation):
        used = int((lengths > 0).sum())
        fixed = max(1, used // 4)
        moved = fixed + (places - fixed + rotation * (used - fixed)) % max(1, count - fixed)
        return jnp.zeros((count,), jnp.int32).at[order[jnp.where(places < fixed, places, moved)]].set(jnp.asarray(lengths, jnp.int32))

    lengths = jnp.where(number % 4 == 0, named(packed, number // 4), named(common, number - number // 4 - 1))
    mixed = jax.random.permutation(jax.random.fold_in(own, 3), count)
    giver, taker = mixed[0:count // 2 * 2:2], mixed[1:count // 2 * 2:2]
    slack = jnp.minimum(lengths[giver] - 1, bound - lengths[taker]) // 2
    slack = jnp.where((giver == order[0]) | (taker == order[0]) | (lengths[taker] == 0), 0, jnp.maximum(slack, 0))
    moved = jax.random.randint(jax.random.fold_in(own, 4), (count // 2,), 0, 1 << 20) % (slack + 1)
    lengths = lengths.at[giver].add(-moved).at[taker].add(moved)
    members = jnp.searchsorted(jnp.cumsum(lengths), jnp.arange(rows * top), side="right").astype(jnp.int32)
    listing = members.reshape(top, rows).T
    listing = listing[jax.random.permutation(jax.random.fold_in(own, 1), rows)]
    rotation = jax.random.randint(jax.random.fold_in(own, 2), (rows, 1), 0, top)
    return jnp.take_along_axis(listing, (jnp.arange(top)[None, :] + rotation) % top, axis=1)


def load_shares(count, total, reach, slope, full):
    portions = [(1 << 20) // math.isqrt(grade ** slope) + 1 for grade in range(1, count + 1)]
    largest = reach if full else min(reach, max(-(-total // count), total * portions[0] // sum(portions)))
    least = 1 if total - largest >= count - 1 else 0
    given, rest = [largest] + [least] * (count - 1), total - largest - least * (count - 1)
    while rest > 0:
        free = [i for i in range(1, count) if given[i] < largest] or [i for i in range(1, count) if given[i] < reach]
        whole, remaining = sum([portions[i] for i in free]), rest
        for i in free:
            extra = min(reach - given[i], max(1, remaining * portions[i] // whole), rest)
            given[i] = given[i] + extra
            rest = rest - extra
    return np.array(given)


def gaussian(rng, dims, deviation, reach, shards=(), kind=jnp.bfloat16):
    gain = block_levels(rng, dims, shards, -0.22, 0.18) if shards else 1.0
    values = jax.random.normal(rng, dims, jnp.float32) * deviation * gain
    return jnp.minimum(jnp.maximum(values, -reach), reach).astype(kind)


def setup_inputs(seed: int = 0, part: int = 0) -> dict:
    key_list = jax.random.split(jax.random.key(seed), 16)
    part_keys = jax.random.split(jax.random.fold_in(key_list[15], part), 16)
    residual = gaussian(part_keys[0], (LEN, SEQS, D), 1.0, 6.0, ((0, 128),))
    query = draw_query(jax.random.fold_in(jax.random.fold_in(key_list[15], part), 71), part)
    latent = gaussian(part_keys[2], (LEN, SEQS, LATENT), 1.0, 6.0, ((0, 16),))
    rope_key = draw_rope_key(jax.random.fold_in(jax.random.fold_in(key_list[15], part), 71), part)
    latent_gain = jnp.clip(1.0 + 0.18 * jax.random.normal(key_list[4], (LATENT,), jnp.float32), 0.1, 1.9)
    key_up = gaussian(key_list[5], (LATENT, HEADS * NOPE), LATENT ** -0.5, 0.25, ((1, 8),))
    value_up = gaussian(key_list[6], (LATENT, HEADS * VDIM), LATENT ** -0.5, 0.25, ((1, 8),))
    out_weight = gaussian(key_list[7], (HEADS * VDIM, D), (HEADS * VDIM // 4) ** -0.5, 0.375, ((0, 8),))
    norm_gain = jnp.clip(1.0 + 0.18 * jax.random.normal(key_list[8], (D,), jnp.float32), 0.1, 1.9)
    group_prob = jnp.clip(jnp.exp(math.log(1.0) - 1.3862944 * jax.random.uniform(part_keys[9], (LEN, SEQS), jnp.float32) ** block_levels(part_keys[9], (LEN, SEQS), ((0, 128),), -0.2, 0.2)), 0.25, 1.0)
    pair_logits = gaussian(part_keys[10], (LEN, SEQS, TOPK), 1.5, 8.0, ((0, 128),), jnp.float32)
    routes_keys = jax.random.split(jax.random.fold_in(part_keys[11], 1), LEN * SEQS // ROWS_DEV)
    routes_turns = jax.random.permutation(jax.random.fold_in(part_keys[11], 3), LEN * SEQS // ROWS_DEV)
    routes = jax.vmap(lambda own, number: assign_block(jax.random.fold_in(part_keys[11], 2), own, number, ROWS_DEV, EXPERTS, TOPK, CAP, 1))(routes_keys, routes_turns).reshape((LEN, SEQS, TOPK))
    w_gate = gaussian(key_list[12], (EXPERTS, D, FF), D ** -0.5, 0.125, ((0, 128),))
    w_up = gaussian(key_list[13], (EXPERTS, D, FF), D ** -0.5, 0.125, ((0, 128),))
    w_down = gaussian(key_list[14], (EXPERTS, FF, D), (FF // 4) ** -0.5, 0.4375, ((0, 128),))
    return {"residual": residual, "query": query, "latent": latent, "rope_key": rope_key, "latent_gain": latent_gain, "key_up": key_up, "value_up": value_up, "out_weight": out_weight, "norm_gain": norm_gain, "group_prob": group_prob, "pair_logits": pair_logits, "routes": routes, "w_gate": w_gate, "w_up": w_up, "w_down": w_down}


epsilon = 1e-06
rotary_base = 10000.0

def rotate(values, positions):
    halfway = values.shape[-1] // 2
    inverse = rotary_base ** (-jnp.arange(halfway, dtype=jnp.float32) / halfway)
    angles = positions.astype(jnp.float32)[:, None] * inverse[None, :]
    angles = angles.reshape((angles.shape[0],) + (1,) * (values.ndim - 2) + (halfway,))
    cosine_values = jnp.cos(angles)
    sine_values = jnp.sin(angles)
    first_half = values[..., :halfway]
    second_half = values[..., halfway:]
    return jnp.concatenate([first_half * cosine_values - second_half * sine_values, second_half * cosine_values + first_half * sine_values], axis=-1)

def rms_scale(values, gain_values):
    return values * lax.rsqrt(lax.optimization_barrier(jnp.mean(values * values, axis=-1, keepdims=True)) + epsilon) * gain_values

def expand(latent_rows, latent_gain, key_up, value_up):
    normed = rms_scale(latent_rows.astype(jnp.float32), latent_gain).astype(jnp.bfloat16)
    keys_nope = jnp.dot(normed, key_up, preferred_element_type=jnp.float32).astype(jnp.bfloat16)
    values = jnp.dot(normed, value_up, preferred_element_type=jnp.float32).astype(jnp.bfloat16)
    lead = latent_rows.shape[:2]
    return (keys_nope.reshape(lead + (key_up.shape[1] // NOPE, NOPE)), values.reshape(lead + (value_up.shape[1] // VDIM, VDIM)))

def reference(residual, query, latent, rope_key, latent_gain, key_up, value_up, out_weight, norm_gain, group_prob, pair_logits, routes, w_gate, w_up, w_down):
    positions = jnp.arange(LEN, dtype=jnp.int32)
    key_nope, value_rows = expand(latent, latent_gain, key_up, value_up)
    key_rot = rotate(rope_key.astype(jnp.float32), positions).astype(jnp.bfloat16)
    split_query = query.reshape(LEN, SEQS, HEADS, QK)
    query_nope = split_query[..., :NOPE]
    query_rot = rotate(split_query[..., NOPE:].astype(jnp.float32), positions).astype(jnp.bfloat16)

    def attend(inputs):
        head_nope, head_rot, head_keys, head_values = inputs
        scores = jnp.einsum('qsd,ksd->sqk', head_nope.astype(jnp.float32), head_keys.astype(jnp.float32))
        scores = scores + jnp.einsum('qsd,ksd->sqk', head_rot.astype(jnp.float32), key_rot.astype(jnp.float32))
        scores = scores * QK ** (-0.5)
        highest = lax.optimization_barrier(jnp.max(scores, axis=-1, keepdims=True))
        weights = jnp.exp(scores - highest)
        totals = lax.optimization_barrier(jnp.sum(weights, axis=-1))
        rounded = lax.optimization_barrier(weights.astype(jnp.bfloat16)).astype(jnp.float32)
        mixed = jnp.einsum('sqk,ksd->sqd', rounded, head_values.astype(jnp.float32))
        return (mixed / totals[..., None]).astype(jnp.bfloat16)
    heads_out = lax.map(attend, (jnp.moveaxis(query_nope, 2, 0), jnp.moveaxis(query_rot, 2, 0), jnp.moveaxis(key_nope, 2, 0), jnp.moveaxis(value_rows, 2, 0)))
    row_total = LEN * SEQS
    attended = jnp.transpose(heads_out, (2, 1, 0, 3)).reshape(row_total, HEADS * VDIM)
    projected = jnp.dot(attended, out_weight, preferred_element_type=jnp.float32)
    stream = (residual.reshape(row_total, D).astype(jnp.float32) + projected).astype(jnp.bfloat16)
    normed = rms_scale(stream.astype(jnp.float32), norm_gain).astype(jnp.bfloat16)
    mixing = jax.nn.softmax(pair_logits.reshape(row_total, TOPK), axis=-1) * group_prob.reshape(row_total, 1)
    blocks = row_total // ROWS_DEV
    chosen = routes.reshape(blocks, ROWS_DEV * TOPK).astype(jnp.int32)
    one_hot = (chosen[..., None] == jnp.arange(EXPERTS, dtype=jnp.int32)).astype(jnp.int32)
    before = jnp.cumsum(one_hot, axis=1) - one_hot
    slot_index = lax.optimization_barrier(jnp.sum(before * one_hot, axis=-1)).astype(jnp.int32)
    column = (jnp.arange(blocks, dtype=jnp.int32)[:, None] * CAP + slot_index).astype(jnp.int32)
    source_row = (jnp.arange(row_total * TOPK, dtype=jnp.int32).reshape(blocks, ROWS_DEV * TOPK) // TOPK).astype(jnp.int32)
    slot_table = jnp.full((EXPERTS, blocks * CAP), row_total, jnp.int32).at[chosen, column].set(source_row)
    padded = jnp.concatenate([normed, jnp.zeros((1, D), jnp.bfloat16)], axis=0)

    def serve_rows(expert_inputs):
        row_numbers, gate_weight, up_weight, down_weight = expert_inputs
        gathered = padded[row_numbers]
        gate_pre = jnp.dot(gathered, gate_weight, preferred_element_type=jnp.float32)
        upward = jnp.dot(gathered, up_weight, preferred_element_type=jnp.float32)
        hidden = (jax.nn.silu(gate_pre) * upward).astype(jnp.bfloat16)
        return jnp.dot(hidden, down_weight, preferred_element_type=jnp.float32).astype(jnp.bfloat16)
    served = lax.map(serve_rows, (slot_table, w_gate, w_up, w_down))
    results = served[chosen, column].reshape(row_total, TOPK, D)
    combined = stream.astype(jnp.float32) + lax.optimization_barrier(jnp.sum(results.astype(jnp.float32) * mixing[..., None], axis=1))
    return combined.astype(jnp.bfloat16).reshape(LEN, SEQS, D)
```

```python
import functools
import math

import jax
import jax.numpy as jnp
from jax import lax
from jax.experimental import pallas as pl
from jax.experimental.pallas import tpu as pltpu
from jax.sharding import PartitionSpec as P

D = 2048
NOPE = 128
VDIM = 128
QK = 192
TOPK = 2
SEQS = 4
CAP = 2
LANES = 128
MESH = pl.DeviceIdType.MESH


epsilon = 1e-06
rotary_base = 10000.0
lowest = -1e30


def side_by_side(arrays, axis, dim, along):
    widths = [math.prod(a.shape[along:]) for a in arrays]
    both = jnp.concatenate(
        [a.reshape(*a.shape[:along], w) for a, w in zip(arrays, widths)], axis=along
    )
    out = lax.all_gather(both, axis, axis=dim, tiled=True)
    pieces = jnp.split(out, [sum(widths[:k]) for k in range(1, len(widths))], axis=along)
    return tuple((b.reshape(*out.shape[:along], *a.shape[along:]) for a, b in zip(arrays, pieces)))


def rotate(values, positions):
    halfway = values.shape[-1] // 2
    inverse = rotary_base ** (-jnp.arange(halfway, dtype=jnp.float32) / halfway)
    angles = positions.astype(jnp.float32)[:, None] * inverse[None, :]
    angles = angles.reshape((angles.shape[0],) + (1,) * (values.ndim - 2) + (halfway,))
    cosine_values = jnp.cos(angles)
    sine_values = jnp.sin(angles)
    first_half = values[..., :halfway]
    second_half = values[..., halfway:]
    return jnp.concatenate(
        [
            first_half * cosine_values - second_half * sine_values,
            second_half * cosine_values + first_half * sine_values,
        ],
        axis=-1,
    )


def rms_scale(values, gain_values):
    return (
        values
        * lax.rsqrt(jnp.mean(values * values, axis=-1, keepdims=True) + epsilon)
        * gain_values
    )


def expand(latent_rows, latent_gain, key_up, value_up):
    normed = rms_scale(latent_rows.astype(jnp.float32), latent_gain).astype(jnp.bfloat16)
    keys_nope = jnp.dot(normed, key_up, preferred_element_type=jnp.float32).astype(jnp.bfloat16)
    values = jnp.dot(normed, value_up, preferred_element_type=jnp.float32).astype(jnp.bfloat16)
    lead = latent_rows.shape[:2]
    return (
        keys_nope.reshape(lead + (key_up.shape[1] // NOPE, NOPE)),
        values.reshape(lead + (value_up.shape[1] // VDIM, VDIM)),
    )


def absorb(carried, query_nope, query_rot, key_nope, value_rows, key_rot):
    running, totals, accumulated = carried
    scores = jnp.einsum("qshd,kshd->qshk", query_nope, key_nope, preferred_element_type=jnp.float32)
    scores = scores + jnp.einsum(
        "qshd,ksd->qshk", query_rot, key_rot, preferred_element_type=jnp.float32
    )
    scores = scores * QK ** (-0.5)
    highest = jnp.maximum(running, jnp.max(scores, axis=-1))
    weights = jnp.exp(scores - highest[..., None])
    totals = jnp.sum(weights, axis=-1)
    accumulated = jnp.einsum(
        "qshk,kshd->qshd",
        weights.astype(jnp.bfloat16),
        value_rows,
        preferred_element_type=jnp.float32,
    )
    return (highest, totals, accumulated)


def moe_kernel(sp_n, tp_n, normed_ref, stream_ref, routes_ref, mix_ref, wg_hbm, wu_hbm, wd_hbm, out_ref,
               wg, wu, wd, stage, outgoing, arrived, leaving, returned, rows_in, w_sems, send_sem, recv_sem, back_send, back_recv):
    peers = sp_n * tp_n
    rows, width = normed_ref.shape
    chunks = width // LANES
    sp, tp = lax.axis_index("sp"), lax.axis_index("tp")
    me = sp * tp_n + tp
    barrier = pltpu.get_barrier_semaphore()

    def peer(i):
        other = lax.rem(me + i, peers)
        return other, {"sp": other // tp_n, "tp": lax.rem(other, tp_n)}

    def greet(i, _):
        pl.semaphore_signal(barrier, inc=1, device_id=peer(i)[1], device_id_type=MESH)
        return 0

    lax.fori_loop(1, peers, greet, 0)
    loads = [
        pltpu.make_async_copy(src, dst, w_sems.at[k])
        for k, (src, dst) in enumerate(((wg_hbm, wg), (wu_hbm, wu), (wd_hbm, wd)))
    ]
    for load in loads:
        load.start()

    experts = lax.broadcasted_iota(jnp.int32, (rows, peers), 1)
    picks = [(routes_ref[:, k : k + 1] == experts).astype(jnp.float32) for k in range(TOPK)]
    both = (picks[0] + picks[1]).astype(jnp.bfloat16)
    earlier = (
        lax.broadcasted_iota(jnp.int32, (rows, rows), 0) > lax.broadcasted_iota(jnp.int32, (rows, rows), 1)
    ).astype(jnp.float32).astype(jnp.bfloat16)
    before = jnp.dot(earlier, both, preferred_element_type=jnp.float32)
    chosen = []
    for pick in picks:
        slot = jnp.sum(pick * before, axis=1, keepdims=True)
        chosen.append(jnp.concatenate([pick * (1.0 - slot), pick * slot], axis=1))
    taken = (chosen[0] + chosen[1]).astype(jnp.bfloat16)
    chosen = [c.astype(jnp.bfloat16) for c in chosen]

    for j in range(chunks // 2):
        part = lax.dot_general(
            taken, normed_ref[:, 2 * j * LANES : (2 * j + 2) * LANES], (((0,), (0,)), ((), ())),
            preferred_element_type=jnp.float32,
        )
        for c in range(CAP):
            for h in range(2):
                stage[pl.ds(c * chunks + 2 * j + h, peers, stride=CAP * chunks), :] = part[
                    c * peers : (c + 1) * peers, h * LANES : (h + 1) * LANES
                ]
    step = min(8, peers)
    span = CAP * chunks

    def pack(dst):
        def body(i, _):
            rows_at = pl.ds(pl.multiple_of(i * step * span, step * span), step * span)
            dst[pl.ds(i * step, step)] = stage[rows_at, :].astype(jnp.bfloat16).reshape(step, span, LANES)
            return 0

        lax.fori_loop(0, peers // step, body, 0)

    def unpack(src):
        def body(i, _):
            rows_at = pl.ds(pl.multiple_of(i * step * span, step * span), step * span)
            stage[rows_at, :] = src[pl.ds(i * step, step)].astype(jnp.float32).reshape(step * span, LANES)
            return 0

        lax.fori_loop(0, peers // step, body, 0)

    def exchange(src, dst, sent, got):
        def body(i, _):
            other, where = peer(i)
            pltpu.make_async_remote_copy(
                src_ref=src.at[other], dst_ref=dst.at[me], send_sem=sent, recv_sem=got, device_id=where,
                device_id_type=MESH,
            ).start()
            return 0

        lax.fori_loop(1, peers, body, 0)
        dst[me] = src[me]

    def settle(buffer, sem):
        many = buffer.at[pl.ds(0, peers - 1)]
        pltpu.make_async_copy(many, many, sem).wait()

    pack(outgoing)
    pl.semaphore_wait(barrier, peers - 1)
    exchange(outgoing, arrived, send_sem, recv_sem)
    for load in loads:
        load.wait()
    settle(arrived, recv_sem)

    unpack(arrived)
    total = peers * CAP
    for l in range(chunks):
        rows_in[:, l * LANES : (l + 1) * LANES] = stage[pl.ds(l, total, stride=chunks), :].astype(jnp.bfloat16)
    tile = 256
    hidden = []
    for j in range(wg.shape[1] // tile):
        cols = slice(j * tile, (j + 1) * tile)
        gate = jnp.dot(rows_in[...], wg[:, cols], preferred_element_type=jnp.float32)
        up = jnp.dot(rows_in[...], wu[:, cols], preferred_element_type=jnp.float32)
        hidden.append((gate / (1.0 + jnp.exp(-gate)) * up).astype(jnp.bfloat16))
    hidden = jnp.concatenate(hidden, axis=1)
    for j in range(chunks // 2):
        part = jnp.dot(hidden, wd[:, 2 * j * LANES : (2 * j + 2) * LANES], preferred_element_type=jnp.float32)
        for h in range(2):
            stage[pl.ds(2 * j + h, total, stride=chunks), :] = part[:, h * LANES : (h + 1) * LANES]
    pack(leaving)
    exchange(leaving, returned, back_send, back_recv)
    settle(outgoing, send_sem)
    settle(returned, back_recv)

    unpack(returned)
    for j in range(chunks // 2):
        block = jnp.concatenate(
            [
                jnp.concatenate(
                    [stage[pl.ds(c * chunks + 2 * j + h, peers, stride=span), :] for c in range(CAP)], axis=0
                )
                for h in range(2)
            ],
            axis=1,
        ).astype(jnp.bfloat16)
        cols = slice(2 * j * LANES, (2 * j + 2) * LANES)
        added = mix_ref[:, 0:1] * jnp.dot(chosen[0], block, preferred_element_type=jnp.float32) + mix_ref[
            :, 1:2
        ] * jnp.dot(chosen[1], block, preferred_element_type=jnp.float32)
        out_ref[:, cols] = (stream_ref[:, cols].astype(jnp.float32) + added).astype(jnp.bfloat16)
    settle(leaving, back_send)


def routed_experts(sp_n, tp_n, normed, stream, routes, mixing, w_gate, w_up, w_down):
    rows, width = normed.shape
    peers = sp_n * tp_n
    span = CAP * width // LANES
    vmem = pl.BlockSpec(memory_space=pltpu.VMEM)
    hbm = pl.BlockSpec(memory_space=pl.ANY)
    blocks = pltpu.VMEM((peers, span, LANES), jnp.bfloat16)
    dma = pltpu.SemaphoreType.DMA
    return pl.pallas_call(
        functools.partial(moe_kernel, sp_n, tp_n),
        out_shape=jax.ShapeDtypeStruct((rows, width), jnp.bfloat16),
        in_specs=[vmem] * 4 + [hbm] * 3,
        out_specs=vmem,
        scratch_shapes=[
            pltpu.VMEM(w_gate.shape, jnp.bfloat16),
            pltpu.VMEM(w_up.shape, jnp.bfloat16),
            pltpu.VMEM(w_down.shape, jnp.bfloat16),
            pltpu.VMEM((peers * span, LANES), jnp.float32),
            blocks, blocks, blocks, blocks,
            pltpu.VMEM((peers * CAP, width), jnp.bfloat16),
            dma((3,)), dma, dma, dma, dma,
        ],
        compiler_params=pltpu.CompilerParams(collective_id=1, has_side_effects=True),
        name="routed_experts",
    )(normed, stream, routes, mixing, w_gate, w_up, w_down)


def shards(
    residual,
    query,
    latent,
    rope_key,
    latent_gain,
    key_up,
    value_up,
    out_weight,
    norm_gain,
    group_prob,
    pair_logits,
    routes,
    w_gate,
    w_up,
    w_down,
):
    positions_here = query.shape[0]
    heads_here = key_up.shape[1] // NOPE
    own_positions = lax.axis_index("sp") * positions_here + jnp.arange(
        positions_here, dtype=jnp.int32
    )
    split_query = query.reshape(positions_here, SEQS, heads_here, QK)
    query_nope = split_query[..., :NOPE]
    query_rot = rotate(split_query[..., NOPE:].astype(jnp.float32), own_positions).astype(
        jnp.bfloat16
    )
    key_rot = rotate(rope_key.astype(jnp.float32), own_positions).astype(jnp.bfloat16)
    initial = (
        jnp.full((positions_here, SEQS, heads_here), lowest, jnp.float32),
        jnp.zeros((positions_here, SEQS, heads_here), jnp.float32),
        jnp.zeros((positions_here, SEQS, heads_here, VDIM), jnp.float32),
    )
    own_keys, own_values = expand(latent, latent_gain, key_up, value_up)
    pieces = side_by_side((own_keys, own_values, key_rot), "sp", 0, 2)
    finished = absorb(initial, query_nope, query_rot, pieces[0], pieces[1], pieces[2])
    attended = (finished[2] / finished[1][..., None]).astype(jnp.bfloat16)
    attended = attended.reshape(positions_here, SEQS, heads_here * VDIM)
    by_token = lax.all_to_all(attended, "tp", split_axis=0, concat_axis=2, tiled=True)
    row_count = by_token.shape[0] * SEQS
    mixed_heads = by_token.reshape(row_count, by_token.shape[2])
    projected = jnp.dot(
        mixed_heads,
        lax.all_gather(out_weight, "tp", axis=0, tiled=True),
        preferred_element_type=jnp.float32,
    )
    stream = (residual.reshape(row_count, D).astype(jnp.float32) + projected).astype(jnp.bfloat16)
    normed = rms_scale(stream.astype(jnp.float32), norm_gain).astype(jnp.bfloat16)
    mixing = jax.nn.softmax(pair_logits.reshape(row_count, TOPK), axis=-1) * group_prob.reshape(
        row_count, 1
    )
    combined = routed_experts(
        lax.axis_size("sp"),
        lax.axis_size("tp"),
        normed,
        stream,
        routes.reshape(row_count, TOPK),
        mixing,
        w_gate[0],
        w_up[0],
        w_down[0],
    )
    return combined.reshape(residual.shape)


def solution(mesh):
    placed = (
        P(("sp", "tp"), "grp", None),
        P("sp", "grp", "tp"),
        P("sp", "grp", None),
        P("sp", "grp", None),
        P(),
        P(None, "tp"),
        P(None, "tp"),
        P("tp", None),
        P(),
        P(("sp", "tp"), "grp"),
        P(("sp", "tp"), "grp", None),
        P(("sp", "tp"), "grp", None),
        P(("sp", "tp"), None, None),
        P(("sp", "tp"), None, None),
        P(("sp", "tp"), None, None),
    )
    return jax.shard_map(
        shards, mesh=mesh, in_specs=placed, out_specs=P(("sp", "tp"), "grp", None), check_vma=False
    )
```

```python
import functools
import math

import jax
import jax.numpy as jnp
from jax import lax
from jax.experimental import pallas as pl
from jax.experimental.pallas import tpu as pltpu
from jax.sharding import PartitionSpec as P

D = 2048
NOPE = 128
QK = 192
TOPK = 2
CAP = 2
LANES = 128
MESH = pl.DeviceIdType.MESH


epsilon = 1e-06
rotary_base = 10000.0


def rotate_by(values, positions):
    halfway = values.shape[-1] // 2
    inverse = rotary_base ** (-jnp.arange(halfway, dtype=jnp.float32) / halfway)
    angles = positions.astype(jnp.float32)[:, None] * inverse[None, :]
    cosine_values = jnp.cos(angles)
    sine_values = jnp.sin(angles)
    first_half = values[..., :halfway]
    second_half = values[..., halfway:]
    return jnp.concatenate(
        [
            first_half * cosine_values - second_half * sine_values,
            second_half * cosine_values + first_half * sine_values,
        ],
        axis=-1,
    )


def rms_scale(values, gain_values):
    return (
        values
        * lax.rsqrt(jnp.mean(values * values, axis=-1, keepdims=True) + epsilon)
        * gain_values
    )


def attention_kernel(sp_n, tp_n, seqs, q_ref, kv_ref, ow_ref, res_ref, gain_ref, stream_ref, normed_ref,
                     kv_all, q_all, ow_all, att, heads_y, heads_in, run_max, run_sum, acc,
                     kv_sem, kv_fwd, kv_sib, q_sem, ow_sem, ow_sib, y_sem, x_sem, kv_sent, q_sent, ow_sent, ow_half, ow_sib_sent, y_sent, x_sent):
    chips = sp_n // 2
    side = chips // 2
    half_ring = tp_n // 2
    sp, tp = lax.axis_index("sp"), lax.axis_index("tp")
    chip, core = sp // 2, lax.rem(sp, 2)
    own_seq, own_g = chip // 2, lax.rem(chip, 2)
    positions = q_ref.shape[1]
    half = positions // 2
    part = ow_ref.shape[0] // 2

    def at(chip_id, core_id=None):
        return {"sp": 2 * chip_id + (core if core_id is None else core_id)}

    homes = []
    for e in range(1, seqs):
        seq = lax.rem(own_seq + e, seqs)
        delta = lax.rem(chip - 2 * seq + chips, chips)
        g = 1 - lax.rem(delta + chips - 1, chips) // side
        home = 2 * seq + g
        k = g * lax.rem(chip - home + chips, chips) + (1 - g) * lax.rem(home - chip + chips, chips)
        homes.append((seq, g, home, k))
    sources = [lax.rem(chip + (2 * own_g - 1) * k + chips, chips) for k in range(side)]
    beside = 2 * own_seq + 1 - own_g
    right, left = lax.rem(tp + 1, tp_n), lax.rem(tp + tp_n - 1, tp_n)

    def slot(core_id, g, k):
        return (core_id * 2 + g) * side + k

    def send(src, dst, sent, got, where):
        pltpu.make_async_remote_copy(
            src_ref=src, dst_ref=dst, send_sem=sent, recv_sem=got, device_id=where, device_id_type=MESH
        ).start()

    def landed(buffer, sem):
        pltpu.make_async_copy(buffer, buffer, sem).wait()

    barrier = pltpu.get_barrier_semaphore()
    peers = [at(h[2]) for h in homes] + [at(s) for s in sources[1:]] + [at(beside), at(chip, 1 - core)]
    peers += [{"tp": lax.rem(tp + d, tp_n)} for d in range(1, tp_n)]
    for where in peers:
        pl.semaphore_signal(barrier, inc=1, device_id=where, device_id_type=MESH)
    pl.semaphore_wait(barrier, len(peers))

    own_slot = slot(core, own_g, 0)
    for seq, g, home, k in homes:
        send(kv_ref.at[seq], kv_all.at[slot(core, g, k)], kv_sent, kv_sem.at[k], at(home))
        send(q_ref.at[seq], q_all.at[k], q_sent, q_sem.at[k], at(home))

    def ow_stage(r):
        for way, to in ((0, right), (1, left)):
            head = lax.rem(tp + (r - 1 if way else 1 - r) + tp_n, tp_n)
            if r < half_ring:
                src = ow_ref.at[pl.ds(core * part, part)] if r == 1 else ow_all.at[head, core]
                send(src, ow_all.at[head, core], ow_sent, ow_sem.at[way, r - 1], {"tp": to})
            else:
                rows = pl.ds(way * (part // 2), part // 2)
                src = ow_ref.at[pl.ds(core * part + way * (part // 2), part // 2)] if r == 1 else ow_all.at[head, core, rows]
                send(src, ow_all.at[head, core, rows], ow_half, ow_sem.at[way, r - 1], {"tp": to})

    def ow_arrived(r):
        for way in range(2):
            head = lax.rem(tp + (r if way else -r) + tp_n, tp_n)
            if r < half_ring:
                landed(ow_all.at[head, core], ow_sem.at[way, r - 1])
            else:
                landed(ow_all.at[head, core, pl.ds(way * (part // 2), part // 2)], ow_sem.at[way, r - 1])
            if r < half_ring or way == 1:
                send(ow_all.at[head, core], ow_all.at[head, core], ow_sib_sent, ow_sib, at(chip, 1 - core))
        if r < half_ring:
            ow_stage(r + 1)

    def pass_on(k, src):
        place = kv_all.at[slot(core, own_g, k)]
        send(src, place, kv_sent, kv_fwd.at[k], at(beside))
        send(src, place, kv_sent, kv_sib.at[own_g, k], at(chip, 1 - core))

    ow_stage(1)
    pass_on(0, kv_ref.at[own_seq])
    kv_all[own_slot] = kv_ref[own_seq]
    q_all[0] = q_ref[own_seq]
    ow_all[tp] = ow_ref[...].reshape(ow_all.shape[1:])

    lane = lax.broadcasted_iota(jnp.int32, (positions, 2 * LANES), 1)
    low = lane < LANES + LANES // 2
    high = (lane < LANES) | (lane >= LANES + LANES // 2)
    factor = QK ** (-0.5) * math.log2(math.e)

    def attend(base, k, first, last):
        def rows(start):
            return kv_all[pl.ds(base, side), start : start + half, :].reshape(side * half, LANES)

        q = q_all[k]
        turned = rows(4 * half)
        scores = []
        for n, mask in ((0, low), (1, high)):
            keys = jnp.concatenate([rows(n * half), turned], axis=1)
            scores.append(
                lax.dot_general(
                    jnp.where(mask, q, jnp.zeros_like(q)), keys, (((1,), (1,)), ((), ())),
                    preferred_element_type=jnp.float32,
                )
            )
        top = jnp.maximum(jnp.max(scores[0], axis=1, keepdims=True), jnp.max(scores[1], axis=1, keepdims=True))
        if not first:
            old = run_max[k][:, :1]
            top = jnp.maximum(top, old)
            shrink = jnp.exp2((old - top) * factor)
        total, mixed = 0.0, 0.0
        for n in range(2):
            weights = jnp.exp2((scores[n] - top) * factor)
            total = total + jnp.sum(weights, axis=1, keepdims=True)
            mixed = mixed + jnp.dot(weights.astype(jnp.bfloat16), rows((2 + n) * half), preferred_element_type=jnp.float32)
        if not first:
            total = total + shrink * run_sum[k][:, :1]
            mixed = mixed + shrink * acc[k]
        if last:
            att[k] = (mixed / total).reshape(att.shape[1:]).astype(jnp.bfloat16)
        else:
            run_max[k] = jnp.broadcast_to(top, run_max.shape[1:])
            run_sum[k] = jnp.broadcast_to(total, run_sum.shape[1:])
            acc[k] = mixed

    def attend_all(base, first):
        def body(k, _):
            attend(base, k, first, False)
            return 0

        lax.fori_loop(0, side, body, 0)

    for k in range(1, side):
        landed(kv_all.at[slot(core, own_g, k)], kv_sem.at[k])
        pass_on(k, kv_all.at[slot(core, own_g, k)])
        if k < half_ring:
            ow_arrived(k)
    for k in range(1, side):
        landed(q_all.at[k], q_sem.at[k])
    attend_all(slot(core, own_g, 0), True)
    for k in range(side):
        landed(kv_all.at[slot(1 - core, own_g, k)], kv_sib.at[own_g, k])
    attend_all(slot(1 - core, own_g, 0), False)
    for k in range(side):
        place = kv_all.at[slot(core, 1 - own_g, k)]
        landed(place, kv_fwd.at[k])
        send(place, place, kv_sent, kv_sib.at[1 - own_g, k], at(chip, 1 - core))
    for r in range(min(side, half_ring), half_ring + 1):
        ow_arrived(r)
    attend_all(slot(core, 1 - own_g, 0), False)
    for k in range(side):
        landed(kv_all.at[slot(1 - core, 1 - own_g, k)], kv_sib.at[1 - own_g, k])
    for k in list(range(1, side)) + [0]:
        attend(slot(1 - core, 1 - own_g, 0), k, False, True)
        if k > 0:
            send(att.at[k], heads_y.at[own_seq], y_sent, y_sem, at(sources[k]))
    heads_y[own_seq] = att[0]
    if seqs > 1:
        landed(heads_y.at[pl.ds(0, seqs - 1)], y_sem)
    for d in range(1, tp_n):
        to = lax.rem(tp + d, tp_n)
        send(heads_y.at[:, to], heads_in.at[tp], x_sent, x_sem, {"tp": to})
    heads_in[tp] = heads_y[:, tp]
    landed(ow_all.at[pl.ds(0, tp_n - 1), 0], ow_sib)
    landed(heads_in.at[pl.ds(0, tp_n - 1)], x_sem)

    rows, width = res_ref.shape
    each = rows // seqs
    lhs = jnp.concatenate(
        [heads_in[h].astype(jnp.float32).reshape(rows, LANES).astype(jnp.bfloat16) for h in range(tp_n)], axis=1
    )
    r_out = lax.broadcasted_iota(jnp.int32, (rows, rows), 0)
    r_in = lax.broadcasted_iota(jnp.int32, (rows, rows), 1)
    shuffle = (r_in == lax.rem(r_out, seqs) * each + r_out // seqs).astype(jnp.float32).astype(jnp.bfloat16)
    lhs = jnp.dot(shuffle, lhs, preferred_element_type=jnp.float32).astype(jnp.bfloat16)
    squares = 0.0
    tile = 2 * LANES
    for j in range(width // tile):
        cols = slice(j * tile, (j + 1) * tile)
        weight = ow_all[:, :, :, cols].reshape(lhs.shape[1], tile)
        summed = res_ref[:, cols].astype(jnp.float32) + jnp.dot(lhs, weight, preferred_element_type=jnp.float32)
        rounded = summed.astype(jnp.bfloat16)
        stream_ref[:, cols] = rounded
        wide = rounded.astype(jnp.float32)
        squares = squares + jnp.sum(wide * wide, axis=1, keepdims=True)
    scale = lax.rsqrt(squares / width + epsilon)
    for j in range(width // tile):
        cols = slice(j * tile, (j + 1) * tile)
        normed_ref[:, cols] = (stream_ref[:, cols].astype(jnp.float32) * scale * gain_ref[:, cols]).astype(jnp.bfloat16)

    landed(kv_all.at[pl.ds(0, 4 * side - 1)], kv_sent)
    if seqs > 1:
        landed(q_all.at[pl.ds(0, seqs - 1)], q_sent)
        landed(att.at[pl.ds(0, side - 1)], y_sent)
    if half_ring > 1:
        landed(ow_all.at[pl.ds(0, 2 * (half_ring - 1)), 0], ow_sent)
    landed(ow_all.at[0, 0], ow_half)
    landed(ow_all.at[pl.ds(0, tp_n - 1), 0], ow_sib_sent)
    landed(heads_in.at[pl.ds(0, tp_n - 1)], x_sent)


def attention(sp_n, tp_n, queries, keyed, out_weight, residual, norm_gain):
    seqs, positions, _ = queries.shape
    rows, width = residual.shape
    side = sp_n // 4
    each = positions // tp_n
    vmem = pl.BlockSpec(memory_space=pltpu.VMEM)
    dma = pltpu.SemaphoreType.DMA
    bf16, f32 = jnp.bfloat16, jnp.float32
    return pl.pallas_call(
        functools.partial(attention_kernel, sp_n, tp_n, seqs),
        out_shape=[jax.ShapeDtypeStruct((rows, width), bf16)] * 2,
        in_specs=[vmem] * 5,
        out_specs=[vmem] * 2,
        scratch_shapes=[
            pltpu.VMEM((4 * side,) + keyed.shape[1:], bf16),
            pltpu.VMEM((side,) + queries.shape[1:], bf16),
            pltpu.VMEM((tp_n, 2, out_weight.shape[0] // 2, width), bf16),
            pltpu.VMEM((side, tp_n, each, LANES), bf16),
            pltpu.VMEM((seqs, tp_n, each, LANES), bf16),
            pltpu.VMEM((tp_n, seqs, each, LANES), bf16),
            pltpu.VMEM((side, positions, LANES), f32),
            pltpu.VMEM((side, positions, LANES), f32),
            pltpu.VMEM((side, positions, LANES), f32),
            dma((side,)), dma((side,)), dma((2, side)), dma((side,)), dma((2, tp_n // 2)),
            dma, dma, dma, dma, dma, dma, dma, dma, dma, dma,
        ],
        compiler_params=pltpu.CompilerParams(collective_id=2, has_side_effects=True),
        name="attention",
    )(queries, keyed, out_weight, residual, norm_gain)


def prepared(query, latent, rope_key, latent_gain, key_up, value_up, own_positions):
    seqs = query.shape[1]
    half = query.shape[0] // 2
    by_seq = query.transpose(1, 0, 2)
    turned = rotate_by(by_seq[..., NOPE:].astype(jnp.float32), own_positions).astype(jnp.bfloat16)
    queries = jnp.concatenate([by_seq[..., :NOPE], turned, turned], axis=-1)
    rows = latent.transpose(1, 0, 2)
    normed = rms_scale(rows.astype(jnp.float32), latent_gain).astype(jnp.bfloat16)
    keys = jnp.dot(normed, key_up, preferred_element_type=jnp.float32).astype(jnp.bfloat16)
    values = jnp.dot(normed, value_up, preferred_element_type=jnp.float32).astype(jnp.bfloat16)
    key_rot = rotate_by(rope_key.transpose(1, 0, 2).astype(jnp.float32), own_positions).astype(jnp.bfloat16)
    packed = jnp.concatenate([key_rot[:, :half], key_rot[:, half:]], axis=-1)
    return queries, jnp.concatenate([keys, values, packed], axis=1)


def moe_kernel(sp_n, tp_n, normed_ref, stream_ref, routes_ref, mix_ref, wg_hbm, wu_hbm, wd_hbm, out_ref,
               wg, wu, wd, stage, outgoing, arrived, leaving, returned, rows_in, w_sems, send_sem, recv_sem, back_send, back_recv):
    peers = sp_n * tp_n
    rows, width = normed_ref.shape
    chunks = width // LANES
    sp, tp = lax.axis_index("sp"), lax.axis_index("tp")
    me = sp * tp_n + tp
    barrier = pltpu.get_barrier_semaphore()

    def peer(i):
        other = lax.rem(me + i, peers)
        return other, {"sp": other // tp_n, "tp": lax.rem(other, tp_n)}

    def greet(i, _):
        pl.semaphore_signal(barrier, inc=1, device_id=peer(i)[1], device_id_type=MESH)
        return 0

    lax.fori_loop(1, peers, greet, 0)
    loads = [
        pltpu.make_async_copy(src, dst, w_sems.at[k])
        for k, (src, dst) in enumerate(((wg_hbm, wg), (wu_hbm, wu), (wd_hbm, wd)))
    ]
    for load in loads:
        load.start()

    experts = lax.broadcasted_iota(jnp.int32, (rows, peers), 1)
    picks = [(routes_ref[:, k : k + 1] == experts).astype(jnp.float32) for k in range(TOPK)]
    both = (picks[0] + picks[1]).astype(jnp.bfloat16)
    earlier = (
        lax.broadcasted_iota(jnp.int32, (rows, rows), 0) > lax.broadcasted_iota(jnp.int32, (rows, rows), 1)
    ).astype(jnp.float32).astype(jnp.bfloat16)
    before = jnp.dot(earlier, both, preferred_element_type=jnp.float32)
    chosen = []
    for pick in picks:
        slot = jnp.sum(pick * before, axis=1, keepdims=True)
        chosen.append(jnp.concatenate([pick * (1.0 - slot), pick * slot], axis=1))
    taken = (chosen[0] + chosen[1]).astype(jnp.bfloat16)
    chosen = [c.astype(jnp.bfloat16) for c in chosen]

    for j in range(chunks // 2):
        part = lax.dot_general(
            taken, normed_ref[:, 2 * j * LANES : (2 * j + 2) * LANES], (((0,), (0,)), ((), ())),
            preferred_element_type=jnp.float32,
        )
        for c in range(CAP):
            for h in range(2):
                stage[pl.ds(c * chunks + 2 * j + h, peers, stride=CAP * chunks), :] = part[
                    c * peers : (c + 1) * peers, h * LANES : (h + 1) * LANES
                ]
    step = min(8, peers)
    span = CAP * chunks

    def pack(dst):
        def body(i, _):
            rows_at = pl.ds(pl.multiple_of(i * step * span, step * span), step * span)
            dst[pl.ds(i * step, step)] = stage[rows_at, :].astype(jnp.bfloat16).reshape(step, span, LANES)
            return 0

        lax.fori_loop(0, peers // step, body, 0)

    def unpack(src):
        def body(i, _):
            rows_at = pl.ds(pl.multiple_of(i * step * span, step * span), step * span)
            stage[rows_at, :] = src[pl.ds(i * step, step)].astype(jnp.float32).reshape(step * span, LANES)
            return 0

        lax.fori_loop(0, peers // step, body, 0)

    def exchange(src, dst, sent, got):
        def body(i, _):
            other, where = peer(i)
            pltpu.make_async_remote_copy(
                src_ref=src.at[other], dst_ref=dst.at[me], send_sem=sent, recv_sem=got, device_id=where,
                device_id_type=MESH,
            ).start()
            return 0

        lax.fori_loop(1, peers, body, 0)
        dst[me] = src[me]

    def settle(buffer, sem):
        many = buffer.at[pl.ds(0, peers - 1)]
        pltpu.make_async_copy(many, many, sem).wait()

    pack(outgoing)
    pl.semaphore_wait(barrier, peers - 1)
    exchange(outgoing, arrived, send_sem, recv_sem)
    for load in loads:
        load.wait()
    settle(arrived, recv_sem)

    unpack(arrived)
    total = peers * CAP
    for l in range(chunks):
        rows_in[:, l * LANES : (l + 1) * LANES] = stage[pl.ds(l, total, stride=chunks), :].astype(jnp.bfloat16)
    tile = 256
    hidden = []
    for j in range(wg.shape[1] // tile):
        cols = slice(j * tile, (j + 1) * tile)
        gate = jnp.dot(rows_in[...], wg[:, cols], preferred_element_type=jnp.float32)
        up = jnp.dot(rows_in[...], wu[:, cols], preferred_element_type=jnp.float32)
        hidden.append((gate / (1.0 + jnp.exp(-gate)) * up).astype(jnp.bfloat16))
    hidden = jnp.concatenate(hidden, axis=1)
    for j in range(chunks // 2):
        part = jnp.dot(hidden, wd[:, 2 * j * LANES : (2 * j + 2) * LANES], preferred_element_type=jnp.float32)
        for h in range(2):
            stage[pl.ds(2 * j + h, total, stride=chunks), :] = part[:, h * LANES : (h + 1) * LANES]
    pack(leaving)
    exchange(leaving, returned, back_send, back_recv)
    settle(outgoing, send_sem)
    settle(returned, back_recv)

    unpack(returned)
    for j in range(chunks // 2):
        block = jnp.concatenate(
            [
                jnp.concatenate(
                    [stage[pl.ds(c * chunks + 2 * j + h, peers, stride=span), :] for c in range(CAP)], axis=0
                )
                for h in range(2)
            ],
            axis=1,
        ).astype(jnp.bfloat16)
        cols = slice(2 * j * LANES, (2 * j + 2) * LANES)
        added = mix_ref[:, 0:1] * jnp.dot(chosen[0], block, preferred_element_type=jnp.float32) + mix_ref[
            :, 1:2
        ] * jnp.dot(chosen[1], block, preferred_element_type=jnp.float32)
        out_ref[:, cols] = (stream_ref[:, cols].astype(jnp.float32) + added).astype(jnp.bfloat16)
    settle(leaving, back_send)


def routed_experts(sp_n, tp_n, normed, stream, routes, mixing, w_gate, w_up, w_down):
    rows, width = normed.shape
    peers = sp_n * tp_n
    span = CAP * width // LANES
    vmem = pl.BlockSpec(memory_space=pltpu.VMEM)
    hbm = pl.BlockSpec(memory_space=pl.ANY)
    blocks = pltpu.VMEM((peers, span, LANES), jnp.bfloat16)
    dma = pltpu.SemaphoreType.DMA
    return pl.pallas_call(
        functools.partial(moe_kernel, sp_n, tp_n),
        out_shape=jax.ShapeDtypeStruct((rows, width), jnp.bfloat16),
        in_specs=[vmem] * 4 + [hbm] * 3,
        out_specs=vmem,
        scratch_shapes=[
            pltpu.VMEM(w_gate.shape, jnp.bfloat16),
            pltpu.VMEM(w_up.shape, jnp.bfloat16),
            pltpu.VMEM(w_down.shape, jnp.bfloat16),
            pltpu.VMEM((peers * span, LANES), jnp.float32),
            blocks, blocks, blocks, blocks,
            pltpu.VMEM((peers * CAP, width), jnp.bfloat16),
            dma((3,)), dma, dma, dma, dma,
        ],
        compiler_params=pltpu.CompilerParams(collective_id=1, has_side_effects=True),
        name="routed_experts",
    )(normed, stream, routes, mixing, w_gate, w_up, w_down)


def shards(
    residual,
    query,
    latent,
    rope_key,
    latent_gain,
    key_up,
    value_up,
    out_weight,
    norm_gain,
    group_prob,
    pair_logits,
    routes,
    w_gate,
    w_up,
    w_down,
):
    positions_here = query.shape[0]
    own_positions = lax.axis_index("sp") * positions_here + jnp.arange(
        positions_here, dtype=jnp.int32
    )
    row_count = residual.shape[0] * residual.shape[1]
    queries, keyed = prepared(query, latent, rope_key, latent_gain, key_up, value_up, own_positions)
    stream, normed = attention(
        lax.axis_size("sp"),
        lax.axis_size("tp"),
        queries,
        keyed,
        out_weight,
        residual.reshape(row_count, D),
        norm_gain.reshape(1, D),
    )
    mixing = jax.nn.softmax(pair_logits.reshape(row_count, TOPK), axis=-1) * group_prob.reshape(
        row_count, 1
    )
    combined = routed_experts(
        lax.axis_size("sp"),
        lax.axis_size("tp"),
        normed,
        stream,
        routes.reshape(row_count, TOPK),
        mixing,
        w_gate[0],
        w_up[0],
        w_down[0],
    )
    return combined.reshape(residual.shape)


def solution(mesh):
    placed = (
        P(("sp", "tp"), "grp", None),
        P("sp", "grp", "tp"),
        P("sp", "grp", None),
        P("sp", "grp", None),
        P(),
        P(None, "tp"),
        P(None, "tp"),
        P("tp", None),
        P(),
        P(("sp", "tp"), "grp"),
        P(("sp", "tp"), "grp", None),
        P(("sp", "tp"), "grp", None),
        P(("sp", "tp"), None, None),
        P(("sp", "tp"), None, None),
        P(("sp", "tp"), None, None),
    )
    return jax.shard_map(
        shards, mesh=mesh, in_specs=placed, out_specs=P(("sp", "tp"), "grp", None), check_vma=False
    )
```

```python
import functools
import math

import jax
import jax.numpy as jnp
from jax import lax
from jax.experimental import pallas as pl
from jax.experimental.pallas import tpu as pltpu
from jax.sharding import PartitionSpec as P

D = 2048
NOPE = 128
QK = 192
TOPK = 2
CAP = 2
LANES = 128
MESH = pl.DeviceIdType.MESH


epsilon = 1e-06
rotary_base = 10000.0


def rotate_by(values, positions):
    halfway = values.shape[-1] // 2
    inverse = rotary_base ** (-jnp.arange(halfway, dtype=jnp.float32) / halfway)
    angles = positions.astype(jnp.float32)[:, None] * inverse[None, :]
    cosine_values = jnp.cos(angles)
    sine_values = jnp.sin(angles)
    first_half = values[..., :halfway]
    second_half = values[..., halfway:]
    return jnp.concatenate(
        [
            first_half * cosine_values - second_half * sine_values,
            second_half * cosine_values + first_half * sine_values,
        ],
        axis=-1,
    )


def rms_scale(values, gain_values):
    return (
        values
        * lax.rsqrt(jnp.mean(values * values, axis=-1, keepdims=True) + epsilon)
        * gain_values
    )


def attention_kernel(sp_n, tp_n, seqs, q_ref, kv_ref, ow_ref, res_ref, gain_ref, stream_ref, normed_ref,
                     kv_all, q_all, ow_all, att, heads_y, heads_in, run_max, run_sum, acc,
                     kv_sem, kv_fwd, kv_sib, q_sem, ow_sem, ow_sib, y_sem, x_sem, kv_sent, q_sent, ow_sent, ow_half, ow_sib_sent, y_sent, x_sent):
    chips = sp_n // 2
    side = chips // 2
    half_ring = tp_n // 2
    sp, tp = lax.axis_index("sp"), lax.axis_index("tp")
    chip, core = sp // 2, lax.rem(sp, 2)
    own_seq, own_g = chip // 2, lax.rem(chip, 2)
    positions = q_ref.shape[1]
    half = positions // 2
    part = ow_ref.shape[0] // 2

    def at(chip_id, core_id=None):
        return {"sp": 2 * chip_id + (core if core_id is None else core_id)}

    homes = []
    for e in range(1, seqs):
        seq = lax.rem(own_seq + e, seqs)
        delta = lax.rem(chip - 2 * seq + chips, chips)
        g = 1 - lax.rem(delta + chips - 1, chips) // side
        home = 2 * seq + g
        k = g * lax.rem(chip - home + chips, chips) + (1 - g) * lax.rem(home - chip + chips, chips)
        homes.append((seq, g, home, k))
    sources = [lax.rem(chip + (2 * own_g - 1) * k + chips, chips) for k in range(side)]
    beside = 2 * own_seq + 1 - own_g
    right, left = lax.rem(tp + 1, tp_n), lax.rem(tp + tp_n - 1, tp_n)

    def slot(core_id, g, k):
        return (core_id * 2 + g) * side + k

    def send(src, dst, sent, got, where):
        pltpu.make_async_remote_copy(
            src_ref=src, dst_ref=dst, send_sem=sent, recv_sem=got, device_id=where, device_id_type=MESH
        ).start()

    def landed(buffer, sem):
        pltpu.make_async_copy(buffer, buffer, sem).wait()

    barrier = pltpu.get_barrier_semaphore()
    peers = [at(h[2]) for h in homes] + [at(s) for s in sources[1:]] + [at(beside), at(chip, 1 - core)]
    peers += [{"tp": lax.rem(tp + d, tp_n)} for d in range(1, tp_n)]
    for where in peers:
        pl.semaphore_signal(barrier, inc=1, device_id=where, device_id_type=MESH)
    pl.semaphore_wait(barrier, len(peers))

    own_slot = slot(core, own_g, 0)
    for seq, g, home, k in homes:
        send(kv_ref.at[seq], kv_all.at[slot(core, g, k)], kv_sent, kv_sem.at[k], at(home))
        send(q_ref.at[seq], q_all.at[k], q_sent, q_sem.at[k], at(home))

    def ow_stage(r):
        for way, to in ((0, right), (1, left)):
            head = lax.rem(tp + (r - 1 if way else 1 - r) + tp_n, tp_n)
            if r < half_ring:
                src = ow_ref.at[pl.ds(core * part, part)] if r == 1 else ow_all.at[head, core]
                send(src, ow_all.at[head, core], ow_sent, ow_sem.at[way, r - 1], {"tp": to})
            else:
                rows = pl.ds(way * (part // 2), part // 2)
                src = ow_ref.at[pl.ds(core * part + way * (part // 2), part // 2)] if r == 1 else ow_all.at[head, core, rows]
                send(src, ow_all.at[head, core, rows], ow_half, ow_sem.at[way, r - 1], {"tp": to})

    def ow_arrived(r):
        for way in range(2):
            head = lax.rem(tp + (r if way else -r) + tp_n, tp_n)
            if r < half_ring:
                landed(ow_all.at[head, core], ow_sem.at[way, r - 1])
            else:
                landed(ow_all.at[head, core, pl.ds(way * (part // 2), part // 2)], ow_sem.at[way, r - 1])
            if r < half_ring or way == 1:
                send(ow_all.at[head, core], ow_all.at[head, core], ow_sib_sent, ow_sib, at(chip, 1 - core))
        if r < half_ring:
            ow_stage(r + 1)

    def pass_on(k, src):
        place = kv_all.at[slot(core, own_g, k)]
        send(src, place, kv_sent, kv_fwd.at[k], at(beside))
        send(src, place, kv_sent, kv_sib.at[own_g, k], at(chip, 1 - core))

    ow_stage(1)
    pass_on(0, kv_ref.at[own_seq])
    kv_all[own_slot] = kv_ref[own_seq]
    q_all[0] = q_ref[own_seq]
    ow_all[tp] = ow_ref[...].reshape(ow_all.shape[1:])

    lane = lax.broadcasted_iota(jnp.int32, (positions, 2 * LANES), 1)
    low = lane < LANES + LANES // 2
    high = (lane < LANES) | (lane >= LANES + LANES // 2)
    factor = QK ** (-0.5) * math.log2(math.e)

    def attend(base, k, first, last):
        def rows(start):
            return kv_all[pl.ds(base, side), start : start + half, :].reshape(side * half, LANES)

        q = q_all[k]
        turned = rows(4 * half)
        scores = []
        for n, mask in ((0, low), (1, high)):
            keys = jnp.concatenate([rows(n * half), turned], axis=1)
            scores.append(
                lax.dot_general(
                    jnp.where(mask, q, jnp.zeros_like(q)), keys, (((1,), (1,)), ((), ())),
                    preferred_element_type=jnp.float32,
                )
            )
        top = jnp.maximum(jnp.max(scores[0], axis=1, keepdims=True), jnp.max(scores[1], axis=1, keepdims=True))
        if not first:
            old = run_max[k][:, :1]
            top = jnp.maximum(top, old)
            shrink = jnp.exp2((old - top) * factor)
        total, mixed = 0.0, 0.0
        for n in range(2):
            weights = jnp.exp2((scores[n] - top) * factor)
            total = total + jnp.sum(weights, axis=1, keepdims=True)
            mixed = mixed + jnp.dot(weights.astype(jnp.bfloat16), rows((2 + n) * half), preferred_element_type=jnp.float32)
        if not first:
            total = total + shrink * run_sum[k][:, :1]
            mixed = mixed + shrink * acc[k]
        if last:
            att[k] = (mixed / total).reshape(att.shape[1:]).astype(jnp.bfloat16)
        else:
            run_max[k] = jnp.broadcast_to(top, run_max.shape[1:])
            run_sum[k] = jnp.broadcast_to(total, run_sum.shape[1:])
            acc[k] = mixed

    def attend_all(base, first):
        def body(k, _):
            attend(base, k, first, False)
            return 0

        lax.fori_loop(0, side, body, 0)

    for k in range(1, side):
        landed(kv_all.at[slot(core, own_g, k)], kv_sem.at[k])
        pass_on(k, kv_all.at[slot(core, own_g, k)])
        if k < half_ring:
            ow_arrived(k)
    for k in range(1, side):
        landed(q_all.at[k], q_sem.at[k])
    attend_all(slot(core, own_g, 0), True)
    for k in range(side):
        landed(kv_all.at[slot(1 - core, own_g, k)], kv_sib.at[own_g, k])
    attend_all(slot(1 - core, own_g, 0), False)
    for k in range(side):
        place = kv_all.at[slot(core, 1 - own_g, k)]
        landed(place, kv_fwd.at[k])
        send(place, place, kv_sent, kv_sib.at[1 - own_g, k], at(chip, 1 - core))
    for r in range(min(side, half_ring), half_ring + 1):
        ow_arrived(r)
    attend_all(slot(core, 1 - own_g, 0), False)
    for k in range(side):
        landed(kv_all.at[slot(1 - core, 1 - own_g, k)], kv_sib.at[1 - own_g, k])
    for k in list(range(1, side)) + [0]:
        attend(slot(1 - core, 1 - own_g, 0), k, False, True)
        if k > 0:
            send(att.at[k], heads_y.at[own_seq], y_sent, y_sem, at(sources[k]))
    heads_y[own_seq] = att[0]
    if seqs > 1:
        landed(heads_y.at[pl.ds(0, seqs - 1)], y_sem)
    for d in range(1, tp_n):
        to = lax.rem(tp + d, tp_n)
        send(heads_y.at[:, to], heads_in.at[tp], x_sent, x_sem, {"tp": to})
    heads_in[tp] = heads_y[:, tp]
    landed(ow_all.at[pl.ds(0, tp_n - 1), 0], ow_sib)
    landed(heads_in.at[pl.ds(0, tp_n - 1)], x_sem)

    rows, width = res_ref.shape
    each = rows // seqs
    lhs = jnp.concatenate(
        [heads_in[h].astype(jnp.float32).reshape(rows, LANES).astype(jnp.bfloat16) for h in range(tp_n)], axis=1
    )
    r_out = lax.broadcasted_iota(jnp.int32, (rows, rows), 0)
    r_in = lax.broadcasted_iota(jnp.int32, (rows, rows), 1)
    shuffle = (r_in == lax.rem(r_out, seqs) * each + r_out // seqs).astype(jnp.float32).astype(jnp.bfloat16)
    lhs = jnp.dot(shuffle, lhs, preferred_element_type=jnp.float32).astype(jnp.bfloat16)
    squares = 0.0
    tile = 2 * LANES
    for j in range(width // tile):
        cols = slice(j * tile, (j + 1) * tile)
        weight = ow_all[:, :, :, cols].reshape(lhs.shape[1], tile)
        summed = res_ref[:, cols].astype(jnp.float32) + jnp.dot(lhs, weight, preferred_element_type=jnp.float32)
        rounded = summed.astype(jnp.bfloat16)
        stream_ref[:, cols] = rounded
        wide = rounded.astype(jnp.float32)
        squares = squares + jnp.sum(wide * wide, axis=1, keepdims=True)
    scale = lax.rsqrt(squares / width + epsilon)
    for j in range(width // tile):
        cols = slice(j * tile, (j + 1) * tile)
        normed_ref[:, cols] = (stream_ref[:, cols].astype(jnp.float32) * scale * gain_ref[:, cols]).astype(jnp.bfloat16)

    landed(kv_all.at[pl.ds(0, 4 * side - 1)], kv_sent)
    if seqs > 1:
        landed(q_all.at[pl.ds(0, seqs - 1)], q_sent)
        landed(att.at[pl.ds(0, side - 1)], y_sent)
    if half_ring > 1:
        landed(ow_all.at[pl.ds(0, 2 * (half_ring - 1)), 0], ow_sent)
    landed(ow_all.at[0, 0], ow_half)
    landed(ow_all.at[pl.ds(0, tp_n - 1), 0], ow_sib_sent)
    landed(heads_in.at[pl.ds(0, tp_n - 1)], x_sent)


def attention(sp_n, tp_n, queries, keyed, out_weight, residual, norm_gain):
    seqs, positions, _ = queries.shape
    rows, width = residual.shape
    side = sp_n // 4
    each = positions // tp_n
    vmem = pl.BlockSpec(memory_space=pltpu.VMEM)
    dma = pltpu.SemaphoreType.DMA
    bf16, f32 = jnp.bfloat16, jnp.float32
    return pl.pallas_call(
        functools.partial(attention_kernel, sp_n, tp_n, seqs),
        out_shape=[jax.ShapeDtypeStruct((rows, width), bf16)] * 2,
        in_specs=[vmem] * 5,
        out_specs=[vmem] * 2,
        scratch_shapes=[
            pltpu.VMEM((4 * side,) + keyed.shape[1:], bf16),
            pltpu.VMEM((side,) + queries.shape[1:], bf16),
            pltpu.VMEM((tp_n, 2, out_weight.shape[0] // 2, width), bf16),
            pltpu.VMEM((side, tp_n, each, LANES), bf16),
            pltpu.VMEM((seqs, tp_n, each, LANES), bf16),
            pltpu.VMEM((tp_n, seqs, each, LANES), bf16),
            pltpu.VMEM((side, positions, LANES), f32),
            pltpu.VMEM((side, positions, LANES), f32),
            pltpu.VMEM((side, positions, LANES), f32),
            dma((side,)), dma((side,)), dma((2, side)), dma((side,)), dma((2, tp_n // 2)),
            dma, dma, dma, dma, dma, dma, dma, dma, dma, dma,
        ],
        compiler_params=pltpu.CompilerParams(collective_id=2, has_side_effects=True),
        name="attention",
    )(queries, keyed, out_weight, residual, norm_gain)


def prepared(query, latent, rope_key, latent_gain, key_up, value_up, own_positions):
    seqs = query.shape[1]
    half = query.shape[0] // 2
    by_seq = query.transpose(1, 0, 2)
    turned = rotate_by(by_seq[..., NOPE:].astype(jnp.float32), own_positions).astype(jnp.bfloat16)
    queries = jnp.concatenate([by_seq[..., :NOPE], turned, turned], axis=-1)
    rows = latent.transpose(1, 0, 2)
    normed = rms_scale(rows.astype(jnp.float32), latent_gain).astype(jnp.bfloat16)
    keys = jnp.dot(normed, key_up, preferred_element_type=jnp.float32).astype(jnp.bfloat16)
    values = jnp.dot(normed, value_up, preferred_element_type=jnp.float32).astype(jnp.bfloat16)
    key_rot = rotate_by(rope_key.transpose(1, 0, 2).astype(jnp.float32), own_positions).astype(jnp.bfloat16)
    packed = jnp.concatenate([key_rot[:, :half], key_rot[:, half:]], axis=-1)
    return queries, jnp.concatenate([keys, values, packed], axis=1)


def moe_kernel(sp_n, tp_n, normed_ref, stream_ref, routes_ref, mix_ref, wg_hbm, wu_hbm, wd_hbm, out_ref,
               wg, wu, wd, stage, rows_in, w_sems, *scratch):
    chips = sp_n // 2
    peers = sp_n * tp_n
    plane = chips * tp_n
    rows, width = normed_ref.shape
    chunks = width // LANES
    span = CAP * chunks
    sp, tp = lax.axis_index("sp"), lax.axis_index("tp")
    chip, core = sp // 2, lax.rem(sp, 2)
    barrier = pltpu.get_barrier_semaphore()
    sibling = {"sp": 2 * chip + 1 - core}

    def across(d):
        to = lax.rem(tp + d, tp_n)
        return to, {"tp": to}

    def along(d):
        to = lax.rem(chip + d, chips)
        return to, {"sp": 2 * to + core}

    ring = []
    for d in range(1, max(chips, tp_n) // 2 + 1):
        for step in (d, -d):
            if d < tp_n and (step > 0 or 2 * d != tp_n) and d <= tp_n // 2:
                ring.append((across, step % tp_n))
            if d < chips and (step > 0 or 2 * d != chips) and d <= chips // 2:
                ring.append((along, step % chips))
    for where in [sibling] + [way(d)[1] for way, d in ring]:
        pl.semaphore_signal(barrier, inc=1, device_id=where, device_id_type=MESH)
    loads = [
        pltpu.make_async_copy(src, dst, w_sems.at[k])
        for k, (src, dst) in enumerate(((wg_hbm, wg), (wu_hbm, wu), (wd_hbm, wd)))
    ]
    for load in loads:
        load.start()

    def send(src, dst, sent, got, where):
        pltpu.make_async_remote_copy(
            src_ref=src, dst_ref=dst, send_sem=sent, recv_sem=got, device_id=where, device_id_type=MESH
        ).start()

    def landed(buffer, sem):
        pltpu.make_async_copy(buffer, buffer, sem).wait()

    def exchange(buffers):
        held, given, by_tp, by_sp, from_even, from_odd, sems = buffers

        def even_first():
            for way, d in ring:
                if way is across:
                    to, where = across(d)
                    send(held.at[0, pl.ds(to * chips, chips)], by_tp.at[tp], sems.at[0], sems.at[1], where)

        def odd_first():
            for way, d in ring:
                if way is along:
                    to, where = along(d)
                    send(held.at[1, pl.ds(to * tp_n, tp_n)], by_sp.at[chip], sems.at[2], sems.at[3], where)

        send(given, held.at[core], sems.at[8], sems.at[9], sibling)
        pl.when(core == 0)(even_first)
        pl.when(core == 1)(odd_first)
        landed(given, sems.at[9])
        pl.when(core == 1)(even_first)
        pl.when(core == 0)(odd_first)
        by_tp[tp] = held[0, pl.ds(tp * chips, chips)]
        by_sp[chip] = held[1, pl.ds(chip * tp_n, tp_n)]
        landed(by_tp.at[pl.ds(0, tp_n - 1)], sems.at[1])
        for way, d in ring:
            if way is along:
                to, where = along(d)
                send(by_tp.at[:, to], from_even.at[chip], sems.at[4], sems.at[5], where)
        landed(by_sp.at[pl.ds(0, chips - 1)], sems.at[3])
        for way, d in ring:
            if way is across:
                to, where = across(d)
                send(by_sp.at[:, to], from_odd.at[tp], sems.at[6], sems.at[7], where)
        from_even[chip] = by_tp[:, chip]
        from_odd[tp] = by_sp[:, tp]
        landed(from_even.at[pl.ds(0, chips - 1)], sems.at[5])
        landed(from_odd.at[pl.ds(0, tp_n - 1)], sems.at[7])

    def sent(buffers):
        held, given, by_tp, by_sp, from_even, from_odd, sems = buffers
        landed(given, sems.at[8])
        landed(by_tp.at[pl.ds(0, tp_n - 1)], sems.at[0])
        landed(by_sp.at[pl.ds(0, chips - 1)], sems.at[2])
        landed(from_even.at[pl.ds(0, chips - 1)], sems.at[4])
        landed(from_odd.at[pl.ds(0, tp_n - 1)], sems.at[6])

    step = min(8, plane)

    def pack(buffers, place):
        held, given = buffers[:2]

        def block(i, to_core):
            c = lax.rem(i, chips) * (1 - core) + i // tp_n * core
            x = i // chips * (1 - core) + lax.rem(i, tp_n) * core
            return stage[pl.ds(pl.multiple_of(place(c, to_core, x) * span, span), span), :].astype(jnp.bfloat16)

        def body(n, _):
            for j in range(step):
                i = n * step + j
                held[core, i] = block(i, core)
                given[i] = block(i, 1 - core)
            return 0

        lax.fori_loop(0, plane // step, body, 0)

    def unpack(buffers, place):
        from_even, from_odd = buffers[4:6]

        def put(where, block):
            stage[pl.ds(pl.multiple_of(where * span, span), span), :] = block.astype(jnp.float32)

        def body(n, _):
            for j in range(step):
                i = n * step + j
                c, x = i // tp_n, lax.rem(i, tp_n)
                put(place(c, 0, x), from_even[c, x])
                put(place(c, 1, x), from_odd[x, c])
            return 0

        lax.fori_loop(0, plane // step, body, 0)

    def device(c, core_id, x):
        return (2 * c + core_id) * tp_n + x

    experts = lax.broadcasted_iota(jnp.int32, (rows, peers), 1)
    picks = [(routes_ref[:, k : k + 1] == experts).astype(jnp.float32) for k in range(TOPK)]
    both = (picks[0] + picks[1]).astype(jnp.bfloat16)
    earlier = (
        lax.broadcasted_iota(jnp.int32, (rows, rows), 0) > lax.broadcasted_iota(jnp.int32, (rows, rows), 1)
    ).astype(jnp.float32).astype(jnp.bfloat16)
    before = jnp.dot(earlier, both, preferred_element_type=jnp.float32)
    chosen = []
    for pick in picks:
        slot = jnp.sum(pick * before, axis=1, keepdims=True)
        chosen.append(jnp.concatenate([pick * (1.0 - slot), pick * slot], axis=1))
    taken = (chosen[0] + chosen[1]).astype(jnp.bfloat16)
    chosen = [c.astype(jnp.bfloat16) for c in chosen]

    for j in range(chunks // 2):
        part = lax.dot_general(
            taken, normed_ref[:, 2 * j * LANES : (2 * j + 2) * LANES], (((0,), (0,)), ((), ())),
            preferred_element_type=jnp.float32,
        )
        for c in range(CAP):
            for h in range(2):
                stage[pl.ds(c * chunks + 2 * j + h, peers, stride=span), :] = part[
                    c * peers : (c + 1) * peers, h * LANES : (h + 1) * LANES
                ]
    there, back = scratch[:7], scratch[7:]
    pack(there, device)
    pl.semaphore_wait(barrier, len(ring) + 1)
    exchange(there)
    for load in loads:
        load.wait()

    unpack(there, device)
    total = peers * CAP
    for l in range(chunks):
        rows_in[:, l * LANES : (l + 1) * LANES] = stage[pl.ds(l, total, stride=chunks), :].astype(jnp.bfloat16)
    tile = 256
    hidden = []
    for j in range(wg.shape[1] // tile):
        cols = slice(j * tile, (j + 1) * tile)
        gate = jnp.dot(rows_in[...], wg[:, cols], preferred_element_type=jnp.float32)
        up = jnp.dot(rows_in[...], wu[:, cols], preferred_element_type=jnp.float32)
        hidden.append((gate / (1.0 + jnp.exp(-gate)) * up).astype(jnp.bfloat16))
    hidden = jnp.concatenate(hidden, axis=1)
    for j in range(chunks // 2):
        part = jnp.dot(hidden, wd[:, 2 * j * LANES : (2 * j + 2) * LANES], preferred_element_type=jnp.float32)
        for h in range(2):
            stage[pl.ds(2 * j + h, total, stride=chunks), :] = part[:, h * LANES : (h + 1) * LANES]
    pack(back, device)
    exchange(back)

    unpack(back, device)
    for j in range(chunks // 2):
        block = jnp.concatenate(
            [
                jnp.concatenate(
                    [stage[pl.ds(c * chunks + 2 * j + h, peers, stride=span), :] for c in range(CAP)], axis=0
                )
                for h in range(2)
            ],
            axis=1,
        ).astype(jnp.bfloat16)
        cols = slice(2 * j * LANES, (2 * j + 2) * LANES)
        added = mix_ref[:, 0:1] * jnp.dot(chosen[0], block, preferred_element_type=jnp.float32) + mix_ref[
            :, 1:2
        ] * jnp.dot(chosen[1], block, preferred_element_type=jnp.float32)
        out_ref[:, cols] = (stream_ref[:, cols].astype(jnp.float32) + added).astype(jnp.bfloat16)
    sent(there)
    sent(back)


def routed_experts(sp_n, tp_n, normed, stream, routes, mixing, w_gate, w_up, w_down):
    rows, width = normed.shape
    peers = sp_n * tp_n
    chips = sp_n // 2
    span = CAP * width // LANES
    vmem = pl.BlockSpec(memory_space=pltpu.VMEM)
    hbm = pl.BlockSpec(memory_space=pl.ANY)
    dma = pltpu.SemaphoreType.DMA

    def blocks(*lead):
        return pltpu.VMEM((*lead, span, LANES), jnp.bfloat16)

    buffers = [
        blocks(2, chips * tp_n), blocks(chips * tp_n), blocks(tp_n, chips), blocks(chips, tp_n), blocks(chips, tp_n),
        blocks(tp_n, chips), dma((10,)),
    ]
    return pl.pallas_call(
        functools.partial(moe_kernel, sp_n, tp_n),
        out_shape=jax.ShapeDtypeStruct((rows, width), jnp.bfloat16),
        in_specs=[vmem] * 4 + [hbm] * 3,
        out_specs=vmem,
        scratch_shapes=[
            pltpu.VMEM(w_gate.shape, jnp.bfloat16),
            pltpu.VMEM(w_up.shape, jnp.bfloat16),
            pltpu.VMEM(w_down.shape, jnp.bfloat16),
            pltpu.VMEM((peers * span, LANES), jnp.float32),
            pltpu.VMEM((peers * CAP, width), jnp.bfloat16),
            dma((3,)),
            *buffers,
            *buffers,
        ],
        compiler_params=pltpu.CompilerParams(collective_id=1, has_side_effects=True),
        name="routed_experts",
    )(normed, stream, routes, mixing, w_gate, w_up, w_down)


def shards(
    residual,
    query,
    latent,
    rope_key,
    latent_gain,
    key_up,
    value_up,
    out_weight,
    norm_gain,
    group_prob,
    pair_logits,
    routes,
    w_gate,
    w_up,
    w_down,
):
    positions_here = query.shape[0]
    own_positions = lax.axis_index("sp") * positions_here + jnp.arange(
        positions_here, dtype=jnp.int32
    )
    row_count = residual.shape[0] * residual.shape[1]
    queries, keyed = prepared(query, latent, rope_key, latent_gain, key_up, value_up, own_positions)
    stream, normed = attention(
        lax.axis_size("sp"),
        lax.axis_size("tp"),
        queries,
        keyed,
        out_weight,
        residual.reshape(row_count, D),
        norm_gain.reshape(1, D),
    )
    mixing = jax.nn.softmax(pair_logits.reshape(row_count, TOPK), axis=-1) * group_prob.reshape(
        row_count, 1
    )
    combined = routed_experts(
        lax.axis_size("sp"),
        lax.axis_size("tp"),
        normed,
        stream,
        routes.reshape(row_count, TOPK),
        mixing,
        w_gate[0],
        w_up[0],
        w_down[0],
    )
    return combined.reshape(residual.shape)


def solution(mesh):
    placed = (
        P(("sp", "tp"), "grp", None),
        P("sp", "grp", "tp"),
        P("sp", "grp", None),
        P("sp", "grp", None),
        P(),
        P(None, "tp"),
        P(None, "tp"),
        P("tp", None),
        P(),
        P(("sp", "tp"), "grp"),
        P(("sp", "tp"), "grp", None),
        P(("sp", "tp"), "grp", None),
        P(("sp", "tp"), None, None),
        P(("sp", "tp"), None, None),
        P(("sp", "tp"), None, None),
    )
    return jax.shard_map(
        shards, mesh=mesh, in_specs=placed, out_specs=P(("sp", "tp"), "grp", None), check_vma=False
    )
```

```python
import functools
import math

import jax
import jax.numpy as jnp
from jax import lax
from jax.experimental import pallas as pl
from jax.experimental.pallas import tpu as pltpu
from jax.sharding import PartitionSpec as P

D = 2048
NOPE = 128
QK = 192
TOPK = 2
CAP = 2
PARTS = 2
LANES = 128
MESH = pl.DeviceIdType.MESH


epsilon = 1e-06
rotary_base = 10000.0


def rotate_by(values, positions):
    halfway = values.shape[-1] // 2
    inverse = rotary_base ** (-jnp.arange(halfway, dtype=jnp.float32) / halfway)
    angles = positions.astype(jnp.float32)[:, None] * inverse[None, :]
    cosine_values = jnp.cos(angles)
    sine_values = jnp.sin(angles)
    first_half = values[..., :halfway]
    second_half = values[..., halfway:]
    return jnp.concatenate(
        [
            first_half * cosine_values - second_half * sine_values,
            second_half * cosine_values + first_half * sine_values,
        ],
        axis=-1,
    )


def rms_scale(values, gain_values):
    return (
        values
        * lax.rsqrt(jnp.mean(values * values, axis=-1, keepdims=True) + epsilon)
        * gain_values
    )


def attention_kernel(sp_n, tp_n, seqs, q_ref, kv_ref, ow_ref, res_ref, gain_ref, stream_ref, normed_ref,
                     kv_all, q_all, ow_all, att, heads_y, heads_in, run_max, run_sum, acc,
                     kv_sem, kv_fwd, kv_sib, q_sem, ow_sem, ow_sib, y_sem, x_sem, kv_sent, q_sent, ow_sent, ow_half, ow_sib_sent, y_sent, x_sent):
    chips = sp_n // 2
    side = chips // 2
    half_ring = tp_n // 2
    sp, tp = lax.axis_index("sp"), lax.axis_index("tp")
    chip, core = sp // 2, lax.rem(sp, 2)
    own_seq, own_g = chip // 2, lax.rem(chip, 2)
    half = q_ref.shape[1] // 3
    positions = 2 * half
    part = ow_ref.shape[0] // 2

    def at(chip_id, core_id=None):
        return {"sp": 2 * chip_id + (core if core_id is None else core_id)}

    homes = []
    for e in range(1, seqs):
        seq = lax.rem(own_seq + e, seqs)
        delta = lax.rem(chip - 2 * seq + chips, chips)
        g = 1 - lax.rem(delta + chips - 1, chips) // side
        home = 2 * seq + g
        k = g * lax.rem(chip - home + chips, chips) + (1 - g) * lax.rem(home - chip + chips, chips)
        homes.append((seq, g, home, k))
    sources = [lax.rem(chip + (2 * own_g - 1) * k + chips, chips) for k in range(side)]
    beside = 2 * own_seq + 1 - own_g
    right, left = lax.rem(tp + 1, tp_n), lax.rem(tp + tp_n - 1, tp_n)

    def slot(core_id, g, k):
        return (core_id * 2 + g) * side + k

    def send(src, dst, sent, got, where):
        pltpu.make_async_remote_copy(
            src_ref=src, dst_ref=dst, send_sem=sent, recv_sem=got, device_id=where, device_id_type=MESH
        ).start()

    def landed(buffer, sem):
        pltpu.make_async_copy(buffer, buffer, sem).wait()

    barrier = pltpu.get_barrier_semaphore()
    peers = [at(h[2]) for h in homes] + [at(s) for s in sources[1:]] + [at(beside), at(chip, 1 - core)]
    peers += [{"tp": lax.rem(tp + d, tp_n)} for d in range(1, tp_n)]
    for where in peers:
        pl.semaphore_signal(barrier, inc=1, device_id=where, device_id_type=MESH)
    pl.semaphore_wait(barrier, len(peers))

    own_slot = slot(core, own_g, 0)
    for seq, g, home, k in homes:
        send(kv_ref.at[seq], kv_all.at[slot(core, g, k)], kv_sent, kv_sem.at[k], at(home))

    def ow_stage(r):
        for way, to in ((0, right), (1, left)):
            head = lax.rem(tp + (r - 1 if way else 1 - r) + tp_n, tp_n)
            if r < half_ring:
                src = ow_ref.at[pl.ds(core * part, part)] if r == 1 else ow_all.at[head, core]
                send(src, ow_all.at[head, core], ow_sent, ow_sem.at[way, r - 1], {"tp": to})
            else:
                rows = pl.ds(way * (part // 2), part // 2)
                src = ow_ref.at[pl.ds(core * part + way * (part // 2), part // 2)] if r == 1 else ow_all.at[head, core, rows]
                send(src, ow_all.at[head, core, rows], ow_half, ow_sem.at[way, r - 1], {"tp": to})

    def ow_arrived(r):
        for way in range(2):
            head = lax.rem(tp + (r if way else -r) + tp_n, tp_n)
            if r < half_ring:
                landed(ow_all.at[head, core], ow_sem.at[way, r - 1])
            else:
                landed(ow_all.at[head, core, pl.ds(way * (part // 2), part // 2)], ow_sem.at[way, r - 1])
            if r < half_ring or way == 1:
                send(ow_all.at[head, core], ow_all.at[head, core], ow_sib_sent, ow_sib, at(chip, 1 - core))
        if r < half_ring:
            ow_stage(r + 1)

    def pass_on(k, src):
        place = kv_all.at[slot(core, own_g, k)]
        send(src, place, kv_sent, kv_fwd.at[k], at(beside))
        send(src, place, kv_sent, kv_sib.at[own_g, k], at(chip, 1 - core))

    pass_on(0, kv_ref.at[own_seq])
    ow_stage(1)
    for seq, g, home, k in homes:
        send(q_ref.at[seq], q_all.at[k], q_sent, q_sem.at[k], at(home))
    kv_all[own_slot] = kv_ref[own_seq]
    q_all[0] = q_ref[own_seq]
    ow_all[tp] = ow_ref[...].reshape(ow_all.shape[1:])

    low = lax.broadcasted_iota(jnp.int32, (half, LANES), 1) < LANES // 2
    factor = QK ** (-0.5) * math.log2(math.e)

    def attend(base, k, first, last):
        def rows(start):
            return kv_all[pl.ds(base, side), start : start + half, :].reshape(side * half, LANES)

        plain = q_all[k, :positions]
        first_rot = q_all[k, positions:].astype(jnp.float32)
        second_rot = pltpu.roll(first_rot, LANES // 2, 1)
        halves = [
            jnp.concatenate([jnp.where(low, first_rot, 0.0), jnp.where(low, second_rot, 0.0)], axis=0),
            jnp.concatenate([jnp.where(low, 0.0, second_rot), jnp.where(low, 0.0, first_rot)], axis=0),
        ]
        turned = rows(4 * half)
        scores = []
        for n in range(2):
            keys = jnp.concatenate([rows(n * half), turned], axis=1)
            q = jnp.concatenate([plain, halves[n].astype(jnp.bfloat16)], axis=1)
            scores.append(
                lax.dot_general(q, keys, (((1,), (1,)), ((), ())), preferred_element_type=jnp.float32)
            )
        top = jnp.maximum(jnp.max(scores[0], axis=1, keepdims=True), jnp.max(scores[1], axis=1, keepdims=True))
        if not first:
            old = run_max[k][:, :1]
            top = jnp.maximum(top, old)
            shrink = jnp.exp2((old - top) * factor)
        total, mixed = 0.0, 0.0
        for n in range(2):
            weights = jnp.exp2((scores[n] - top) * factor)
            total = total + jnp.sum(weights, axis=1, keepdims=True)
            mixed = mixed + jnp.dot(weights.astype(jnp.bfloat16), rows((2 + n) * half), preferred_element_type=jnp.float32)
        if not first:
            total = total + shrink * run_sum[k][:, :1]
            mixed = mixed + shrink * acc[k]
        if last:
            att[k] = (mixed / total).reshape(att.shape[1:]).astype(jnp.bfloat16)
        else:
            run_max[k] = jnp.broadcast_to(top, run_max.shape[1:])
            run_sum[k] = jnp.broadcast_to(total, run_sum.shape[1:])
            acc[k] = mixed

    def attend_all(base, first):
        def body(k, _):
            attend(base, k, first, False)
            return 0

        lax.fori_loop(0, side, body, 0)

    def direct_arrived(k):
        place = kv_all.at[slot(core, own_g, k)]
        landed(place, kv_sem.at[k])
        pass_on(k, place)

    def forward_arrived(k):
        place = kv_all.at[slot(core, 1 - own_g, k)]
        landed(place, kv_fwd.at[k])
        send(place, place, kv_sent, kv_sib.at[1 - own_g, k], at(chip, 1 - core))

    forward_arrived(0)
    for k in range(1, side):
        direct_arrived(k)
        if k == 1:
            ow_arrived(1)
        forward_arrived(k)
    for r in range(2, min(3, half_ring + 1)):
        ow_arrived(r)
    for k in range(1, side):
        landed(q_all.at[k], q_sem.at[k])
    attend_all(slot(core, own_g, 0), True)
    for k in range(side):
        landed(kv_all.at[slot(1 - core, own_g, k)], kv_sib.at[own_g, k])
    attend_all(slot(1 - core, own_g, 0), False)
    for r in range(3, half_ring):
        ow_arrived(r)
    attend_all(slot(core, 1 - own_g, 0), False)
    for k in range(side):
        landed(kv_all.at[slot(1 - core, 1 - own_g, k)], kv_sib.at[1 - own_g, k])
    for k in reversed(range(side)):
        attend(slot(1 - core, 1 - own_g, 0), k, False, True)
        if k > 0:
            send(att.at[k], heads_y.at[own_seq], y_sent, y_sem.at[own_seq], at(sources[k]))
    for e in range(seqs):
        seq, block = own_seq, att.at[0]
        if e > 0:
            seq = homes[e - 1][0]
            block = heads_y.at[seq]
            landed(block, y_sem.at[seq])
        for d in range(1, tp_n):
            to = lax.rem(tp + d, tp_n)
            send(block.at[to], heads_in.at[tp, seq], x_sent, x_sem, {"tp": to})
        heads_in[tp, seq] = block[tp]
    if half_ring > 2:
        ow_arrived(half_ring)
    landed(ow_all.at[pl.ds(0, tp_n - 1), 0], ow_sib)
    landed(heads_in.at[pl.ds(0, tp_n - 1)], x_sem)

    rows, width = res_ref.shape
    each = rows // seqs
    lhs = jnp.concatenate(
        [heads_in[h].astype(jnp.float32).reshape(rows, LANES).astype(jnp.bfloat16) for h in range(tp_n)], axis=1
    )
    r_out = lax.broadcasted_iota(jnp.int32, (rows, rows), 0)
    r_in = lax.broadcasted_iota(jnp.int32, (rows, rows), 1)
    shuffle = (r_in == lax.rem(r_out, seqs) * each + r_out // seqs).astype(jnp.float32).astype(jnp.bfloat16)
    lhs = jnp.dot(shuffle, lhs, preferred_element_type=jnp.float32).astype(jnp.bfloat16)
    squares = 0.0
    tile = 2 * LANES
    for j in range(width // tile):
        cols = slice(j * tile, (j + 1) * tile)
        weight = ow_all[:, :, :, cols].reshape(lhs.shape[1], tile)
        summed = res_ref[:, cols].astype(jnp.float32) + jnp.dot(lhs, weight, preferred_element_type=jnp.float32)
        rounded = summed.astype(jnp.bfloat16)
        stream_ref[:, cols] = rounded
        wide = rounded.astype(jnp.float32)
        squares = squares + jnp.sum(wide * wide, axis=1, keepdims=True)
    scale = lax.rsqrt(squares / width + epsilon)
    for j in range(width // tile):
        cols = slice(j * tile, (j + 1) * tile)
        normed_ref[:, cols] = (stream_ref[:, cols].astype(jnp.float32) * scale * gain_ref[:, cols]).astype(jnp.bfloat16)

    landed(kv_all.at[pl.ds(0, 4 * side - 1)], kv_sent)
    if seqs > 1:
        landed(q_all.at[pl.ds(0, seqs - 1)], q_sent)
        landed(att.at[pl.ds(0, side - 1)], y_sent)
    if half_ring > 1:
        landed(ow_all.at[pl.ds(0, 2 * (half_ring - 1)), 0], ow_sent)
    landed(ow_all.at[0, 0], ow_half)
    landed(ow_all.at[pl.ds(0, tp_n - 1), 0], ow_sib_sent)
    landed(heads_in.at[pl.ds(0, tp_n - 1)], x_sent)


def attention(sp_n, tp_n, queries, keyed, out_weight, residual, norm_gain):
    seqs, positions = queries.shape[0], queries.shape[1] // 3 * 2
    rows, width = residual.shape
    side = sp_n // 4
    each = positions // tp_n
    vmem = pl.BlockSpec(memory_space=pltpu.VMEM)
    dma = pltpu.SemaphoreType.DMA
    bf16, f32 = jnp.bfloat16, jnp.float32
    return pl.pallas_call(
        functools.partial(attention_kernel, sp_n, tp_n, seqs),
        out_shape=[jax.ShapeDtypeStruct((rows, width), bf16)] * 2,
        in_specs=[vmem] * 5,
        out_specs=[vmem] * 2,
        scratch_shapes=[
            pltpu.VMEM((4 * side,) + keyed.shape[1:], bf16),
            pltpu.VMEM((side,) + queries.shape[1:], bf16),
            pltpu.VMEM((tp_n, 2, out_weight.shape[0] // 2, width), bf16),
            pltpu.VMEM((side, tp_n, each, LANES), bf16),
            pltpu.VMEM((seqs, tp_n, each, LANES), bf16),
            pltpu.VMEM((tp_n, seqs, each, LANES), bf16),
            pltpu.VMEM((side, positions, LANES), f32),
            pltpu.VMEM((side, positions, LANES), f32),
            pltpu.VMEM((side, positions, LANES), f32),
            dma((side,)), dma((side,)), dma((2, side)), dma((side,)), dma((2, tp_n // 2)),
            dma, dma((seqs,)), dma, dma, dma, dma, dma, dma, dma, dma,
        ],
        compiler_params=pltpu.CompilerParams(collective_id=2, has_side_effects=True),
        name="attention",
    )(queries, keyed, out_weight, residual, norm_gain)


def prepared(query, latent, rope_key, latent_gain, key_up, value_up, own_positions):
    seqs = query.shape[1]
    half = query.shape[0] // 2
    by_seq = query.transpose(1, 0, 2)
    turned = rotate_by(by_seq[..., NOPE:].astype(jnp.float32), own_positions).astype(jnp.bfloat16)
    turned = jnp.concatenate([turned[:, :half], turned[:, half:]], axis=-1)
    queries = jnp.concatenate([by_seq[..., :NOPE], turned], axis=1)
    rows = latent.transpose(1, 0, 2)
    normed = rms_scale(rows.astype(jnp.float32), latent_gain).astype(jnp.bfloat16)
    keys = jnp.dot(normed, key_up, preferred_element_type=jnp.float32).astype(jnp.bfloat16)
    values = jnp.dot(normed, value_up, preferred_element_type=jnp.float32).astype(jnp.bfloat16)
    key_rot = rotate_by(rope_key.transpose(1, 0, 2).astype(jnp.float32), own_positions).astype(jnp.bfloat16)
    packed = jnp.concatenate([key_rot[:, :half], key_rot[:, half:]], axis=-1)
    return queries, jnp.concatenate([keys, values, packed], axis=1)


def moe_kernel(sp_n, tp_n, normed_ref, stream_ref, small_ref, wg_hbm, wu_hbm, wd_hbm, out_ref,
               wg, wu, wd, stage, rows_in, w_sems, *scratch):
    chips = sp_n // 2
    peers = sp_n * tp_n
    plane = chips * tp_n
    rows, width = normed_ref.shape
    chunks = width // LANES
    span = CAP * chunks
    sp, tp = lax.axis_index("sp"), lax.axis_index("tp")
    chip, core = sp // 2, lax.rem(sp, 2)
    barrier = pltpu.get_barrier_semaphore()
    sibling = {"sp": 2 * chip + 1 - core}

    def across(d):
        to = lax.rem(tp + d, tp_n)
        return to, {"tp": to}

    def along(d):
        to = lax.rem(chip + d, chips)
        return to, {"sp": 2 * to + core}

    ring = []
    for d in reversed(range(1, max(chips, tp_n) // 2 + 1)):
        for step in (d, -d):
            if d < tp_n and (step > 0 or 2 * d != tp_n) and d <= tp_n // 2:
                ring.append((across, step % tp_n))
            if d < chips and (step > 0 or 2 * d != chips) and d <= chips // 2:
                ring.append((along, step % chips))
    for where in [sibling] + [way(d)[1] for way, d in ring]:
        pl.semaphore_signal(barrier, inc=1, device_id=where, device_id_type=MESH)
    loads = [
        pltpu.make_async_copy(src, dst, w_sems.at[k])
        for k, (src, dst) in enumerate(((wg_hbm, wg), (wu_hbm, wu), (wd_hbm, wd)))
    ]
    for load in loads:
        load.start()

    def send(src, dst, sent, got, where):
        pltpu.make_async_remote_copy(
            src_ref=src, dst_ref=dst, send_sem=sent, recv_sem=got, device_id=where, device_id_type=MESH
        ).start()

    def landed(buffer, sem):
        pltpu.make_async_copy(buffer, buffer, sem).wait()

    piece = span // PARTS

    def exchange(buffers):
        held, given, by_tp, by_sp, from_even, from_odd, sems, swap = buffers

        def part(p):
            return pl.ds(p * piece, piece)

        def even_first():
            for p in range(PARTS):
                for way, d in ring:
                    if way is across:
                        to, where = across(d)
                        src = held.at[0, pl.ds(to * chips, chips), part(p)]
                        send(src, by_tp.at[tp, :, part(p)], sems.at[p, 0], sems.at[p, 1], where)

        def odd_first():
            for p in range(PARTS):
                for way, d in ring:
                    if way is along:
                        to, where = along(d)
                        src = held.at[1, pl.ds(to * tp_n, tp_n), part(p)]
                        send(src, by_sp.at[chip, :, part(p)], sems.at[p, 2], sems.at[p, 3], where)

        send(given, held.at[core], swap.at[0], swap.at[1], sibling)
        pl.when(core == 0)(even_first)
        pl.when(core == 1)(odd_first)
        landed(given, swap.at[1])
        pl.when(core == 1)(even_first)
        pl.when(core == 0)(odd_first)
        by_tp[tp] = held[0, pl.ds(tp * chips, chips)]
        by_sp[chip] = held[1, pl.ds(chip * tp_n, tp_n)]
        for p in range(PARTS):
            landed(by_tp.at[pl.ds(0, tp_n - 1), :, part(p)], sems.at[p, 1])
            for way, d in ring:
                if way is along:
                    to, where = along(d)
                    send(by_tp.at[:, to, part(p)], from_even.at[chip, :, part(p)], sems.at[p, 4], sems.at[p, 5], where)
            landed(by_sp.at[pl.ds(0, chips - 1), :, part(p)], sems.at[p, 3])
            for way, d in ring:
                if way is across:
                    to, where = across(d)
                    send(by_sp.at[:, to, part(p)], from_odd.at[tp, :, part(p)], sems.at[p, 6], sems.at[p, 7], where)
        from_even[chip] = by_tp[:, chip]
        from_odd[tp] = by_sp[:, tp]
        for p in range(PARTS):
            landed(from_even.at[pl.ds(0, chips - 1), :, part(p)], sems.at[p, 5])
            landed(from_odd.at[pl.ds(0, tp_n - 1), :, part(p)], sems.at[p, 7])

    def sent(buffers):
        held, given, by_tp, by_sp, from_even, from_odd, sems, swap = buffers
        landed(given, swap.at[0])
        for p in range(PARTS):
            part = pl.ds(p * piece, piece)
            landed(by_tp.at[pl.ds(0, tp_n - 1), :, part], sems.at[p, 0])
            landed(by_sp.at[pl.ds(0, chips - 1), :, part], sems.at[p, 2])
            landed(from_even.at[pl.ds(0, chips - 1), :, part], sems.at[p, 4])
            landed(from_odd.at[pl.ds(0, tp_n - 1), :, part], sems.at[p, 6])

    step = min(8, plane)

    def pack(buffers, place):
        held, given = buffers[:2]

        def block(i, to_core):
            c = lax.rem(i, chips) * (1 - core) + i // tp_n * core
            x = i // chips * (1 - core) + lax.rem(i, tp_n) * core
            return stage[pl.ds(pl.multiple_of(place(c, to_core, x) * span, span), span), :].astype(jnp.bfloat16)

        def body(n, _):
            for j in range(step):
                i = n * step + j
                held[core, i] = block(i, core)
                given[i] = block(i, 1 - core)
            return 0

        lax.fori_loop(0, plane // step, body, 0)

    def unpack(buffers, place):
        from_even, from_odd = buffers[4:6]

        def put(where, block):
            stage[pl.ds(pl.multiple_of(where * span, span), span), :] = block.astype(jnp.float32)

        def body(n, _):
            for j in range(step):
                i = n * step + j
                c, x = i // tp_n, lax.rem(i, tp_n)
                put(place(c, 0, x), from_even[c, x])
                put(place(c, 1, x), from_odd[x, c])
            return 0

        lax.fori_loop(0, plane // step, body, 0)

    def device(c, core_id, x):
        return (2 * c + core_id) * tp_n + x

    experts = lax.broadcasted_iota(jnp.int32, (rows, peers), 1).astype(jnp.float32)
    small = small_ref[...]
    picks = [(small[:, k : k + 1] == experts).astype(jnp.float32) for k in range(TOPK)]
    logits = [small[:, TOPK + k : TOPK + k + 1] for k in range(TOPK)]
    top = jnp.maximum(logits[0], logits[1])
    raised = [jnp.exp(v - top) for v in logits]
    shared = small[:, 2 * TOPK : 2 * TOPK + 1]
    mixing = [v / (raised[0] + raised[1]) * shared for v in raised]
    both = (picks[0] + picks[1]).astype(jnp.bfloat16)
    earlier = (
        lax.broadcasted_iota(jnp.int32, (rows, rows), 0) > lax.broadcasted_iota(jnp.int32, (rows, rows), 1)
    ).astype(jnp.float32).astype(jnp.bfloat16)
    before = jnp.dot(earlier, both, preferred_element_type=jnp.float32)
    chosen = []
    for pick in picks:
        slot = jnp.sum(pick * before, axis=1, keepdims=True)
        chosen.append(jnp.concatenate([pick * (1.0 - slot), pick * slot], axis=1))
    taken = (chosen[0] + chosen[1]).astype(jnp.bfloat16)
    chosen = [c.astype(jnp.bfloat16) for c in chosen]

    for j in range(chunks // 2):
        part = lax.dot_general(
            taken, normed_ref[:, 2 * j * LANES : (2 * j + 2) * LANES], (((0,), (0,)), ((), ())),
            preferred_element_type=jnp.float32,
        )
        for c in range(CAP):
            for h in range(2):
                stage[pl.ds(c * chunks + 2 * j + h, peers, stride=span), :] = part[
                    c * peers : (c + 1) * peers, h * LANES : (h + 1) * LANES
                ]
    there, back = scratch[:8], scratch[8:]
    pack(there, device)
    pl.semaphore_wait(barrier, len(ring) + 1)
    exchange(there)
    for load in loads:
        load.wait()

    unpack(there, device)
    total = peers * CAP
    for l in range(chunks):
        rows_in[:, l * LANES : (l + 1) * LANES] = stage[pl.ds(l, total, stride=chunks), :].astype(jnp.bfloat16)
    tile = 256
    hidden = []
    for j in range(wg.shape[1] // tile):
        cols = slice(j * tile, (j + 1) * tile)
        gate = jnp.dot(rows_in[...], wg[:, cols], preferred_element_type=jnp.float32)
        up = jnp.dot(rows_in[...], wu[:, cols], preferred_element_type=jnp.float32)
        hidden.append((gate / (1.0 + jnp.exp(-gate)) * up).astype(jnp.bfloat16))
    hidden = jnp.concatenate(hidden, axis=1)
    for j in range(chunks // 2):
        part = jnp.dot(hidden, wd[:, 2 * j * LANES : (2 * j + 2) * LANES], preferred_element_type=jnp.float32)
        for h in range(2):
            stage[pl.ds(2 * j + h, total, stride=chunks), :] = part[:, h * LANES : (h + 1) * LANES]
    pack(back, device)
    exchange(back)

    unpack(back, device)
    for j in range(chunks // 2):
        block = jnp.concatenate(
            [
                jnp.concatenate(
                    [stage[pl.ds(c * chunks + 2 * j + h, peers, stride=span), :] for c in range(CAP)], axis=0
                )
                for h in range(2)
            ],
            axis=1,
        ).astype(jnp.bfloat16)
        cols = slice(2 * j * LANES, (2 * j + 2) * LANES)
        added = mixing[0] * jnp.dot(chosen[0], block, preferred_element_type=jnp.float32) + mixing[
            1
        ] * jnp.dot(chosen[1], block, preferred_element_type=jnp.float32)
        out_ref[:, cols] = (stream_ref[:, cols].astype(jnp.float32) + added).astype(jnp.bfloat16)
    sent(there)
    sent(back)


def routed_experts(sp_n, tp_n, normed, stream, small, w_gate, w_up, w_down):
    rows, width = normed.shape
    peers = sp_n * tp_n
    chips = sp_n // 2
    span = CAP * width // LANES
    vmem = pl.BlockSpec(memory_space=pltpu.VMEM)
    hbm = pl.BlockSpec(memory_space=pl.ANY)
    dma = pltpu.SemaphoreType.DMA

    def blocks(*lead):
        return pltpu.VMEM((*lead, span, LANES), jnp.bfloat16)

    buffers = [
        blocks(2, chips * tp_n), blocks(chips * tp_n), blocks(tp_n, chips), blocks(chips, tp_n), blocks(chips, tp_n),
        blocks(tp_n, chips), dma((PARTS, 8)), dma((2,)),
    ]
    return pl.pallas_call(
        functools.partial(moe_kernel, sp_n, tp_n),
        out_shape=jax.ShapeDtypeStruct((rows, width), jnp.bfloat16),
        in_specs=[vmem] * 3 + [hbm] * 3,
        out_specs=vmem,
        scratch_shapes=[
            pltpu.VMEM(w_gate.shape, jnp.bfloat16),
            pltpu.VMEM(w_up.shape, jnp.bfloat16),
            pltpu.VMEM(w_down.shape, jnp.bfloat16),
            pltpu.VMEM((peers * span, LANES), jnp.float32),
            pltpu.VMEM((peers * CAP, width), jnp.bfloat16),
            dma((3,)),
            *buffers,
            *buffers,
        ],
        compiler_params=pltpu.CompilerParams(collective_id=1, has_side_effects=True),
        name="routed_experts",
    )(normed, stream, small, w_gate, w_up, w_down)


def shards(
    residual,
    query,
    latent,
    rope_key,
    latent_gain,
    key_up,
    value_up,
    out_weight,
    norm_gain,
    group_prob,
    pair_logits,
    routes,
    w_gate,
    w_up,
    w_down,
):
    positions_here = query.shape[0]
    own_positions = lax.axis_index("sp") * positions_here + jnp.arange(
        positions_here, dtype=jnp.int32
    )
    row_count = residual.shape[0] * residual.shape[1]
    queries, keyed = prepared(query, latent, rope_key, latent_gain, key_up, value_up, own_positions)
    stream, normed = attention(
        lax.axis_size("sp"),
        lax.axis_size("tp"),
        queries,
        keyed,
        out_weight,
        residual.reshape(row_count, D),
        norm_gain.reshape(1, D),
    )
    small = jnp.concatenate([routes.astype(jnp.float32), pair_logits, group_prob[..., None]], axis=-1)
    combined = routed_experts(
        lax.axis_size("sp"),
        lax.axis_size("tp"),
        normed,
        stream,
        small.reshape(row_count, 2 * TOPK + 1),
        w_gate[0],
        w_up[0],
        w_down[0],
    )
    return combined.reshape(residual.shape)


def solution(mesh):
    placed = (
        P(("sp", "tp"), "grp", None),
        P("sp", "grp", "tp"),
        P("sp", "grp", None),
        P("sp", "grp", None),
        P(),
        P(None, "tp"),
        P(None, "tp"),
        P("tp", None),
        P(),
        P(("sp", "tp"), "grp"),
        P(("sp", "tp"), "grp", None),
        P(("sp", "tp"), "grp", None),
        P(("sp", "tp"), None, None),
        P(("sp", "tp"), None, None),
        P(("sp", "tp"), None, None),
    )
    return jax.shard_map(
        shards, mesh=mesh, in_specs=placed, out_specs=P(("sp", "tp"), "grp", None), check_vma=False
    )
```

```python
import functools
import math

import jax
import jax.numpy as jnp
from jax import lax
from jax.experimental import pallas as pl
from jax.experimental.pallas import tpu as pltpu
from jax.sharding import PartitionSpec as P

D = 2048
NOPE = 128
QK = 192
TOPK = 2
CAP = 2
LANES = 128
MESH = pl.DeviceIdType.MESH


epsilon = 1e-06
rotary_base = 10000.0


def rotate_by(values, positions):
    halfway = values.shape[-1] // 2
    inverse = rotary_base ** (-jnp.arange(halfway, dtype=jnp.float32) / halfway)
    angles = positions.astype(jnp.float32)[:, None] * inverse[None, :]
    cosine_values = jnp.cos(angles)
    sine_values = jnp.sin(angles)
    first_half = values[..., :halfway]
    second_half = values[..., halfway:]
    return jnp.concatenate(
        [
            first_half * cosine_values - second_half * sine_values,
            second_half * cosine_values + first_half * sine_values,
        ],
        axis=-1,
    )


def rms_scale(values, gain_values):
    return (
        values
        * lax.rsqrt(jnp.mean(values * values, axis=-1, keepdims=True) + epsilon)
        * gain_values
    )


def attention_kernel(sp_n, tp_n, seqs, q_ref, kv_ref, ow_ref, res_ref, gain_ref, stream_ref, normed_ref,
                     kv_all, q_all, ow_all, att, heads_y, heads_in, run_max, run_sum, acc,
                     kv_sem, kv_fwd, kv_sib, q_sem, ow_sem, ow_sib, y_sem, x_sem, kv_sent, q_sent, ow_sent, ow_half, ow_sib_sent, y_sent, x_sent):
    chips = sp_n // 2
    side = chips // 2
    half_ring = tp_n // 2
    sp, tp = lax.axis_index("sp"), lax.axis_index("tp")
    chip, core = sp // 2, lax.rem(sp, 2)
    own_seq, own_g = chip // 2, lax.rem(chip, 2)
    half = q_ref.shape[1] // 3
    positions = 2 * half
    part = ow_ref.shape[0] // 2

    def at(chip_id, core_id=None):
        return {"sp": 2 * chip_id + (core if core_id is None else core_id)}

    homes = []
    for e in range(1, seqs):
        seq = lax.rem(own_seq + e, seqs)
        delta = lax.rem(chip - 2 * seq + chips, chips)
        g = 1 - lax.rem(delta + chips - 1, chips) // side
        home = 2 * seq + g
        k = g * lax.rem(chip - home + chips, chips) + (1 - g) * lax.rem(home - chip + chips, chips)
        homes.append((seq, g, home, k))
    sources = [lax.rem(chip + (2 * own_g - 1) * k + chips, chips) for k in range(side)]
    beside = 2 * own_seq + 1 - own_g
    right, left = lax.rem(tp + 1, tp_n), lax.rem(tp + tp_n - 1, tp_n)

    def slot(core_id, g, k):
        return (core_id * 2 + g) * side + k

    def send(src, dst, sent, got, where):
        pltpu.make_async_remote_copy(
            src_ref=src, dst_ref=dst, send_sem=sent, recv_sem=got, device_id=where, device_id_type=MESH
        ).start()

    def landed(buffer, sem):
        pltpu.make_async_copy(buffer, buffer, sem).wait()

    barrier = pltpu.get_barrier_semaphore()
    peers = [at(h[2]) for h in homes] + [at(s) for s in sources[1:]] + [at(beside), at(chip, 1 - core)]
    peers += [{"tp": lax.rem(tp + d, tp_n)} for d in range(1, tp_n)]
    for where in peers:
        pl.semaphore_signal(barrier, inc=1, device_id=where, device_id_type=MESH)
    pl.semaphore_wait(barrier, len(peers))

    own_slot = slot(core, own_g, 0)
    for seq, g, home, k in homes:
        send(kv_ref.at[seq], kv_all.at[slot(core, g, k)], kv_sent, kv_sem.at[k], at(home))

    def ow_stage(r):
        for way, to in ((0, right), (1, left)):
            head = lax.rem(tp + (r - 1 if way else 1 - r) + tp_n, tp_n)
            if r < half_ring:
                src = ow_ref.at[pl.ds(core * part, part)] if r == 1 else ow_all.at[head, core]
                send(src, ow_all.at[head, core], ow_sent, ow_sem.at[way, r - 1], {"tp": to})
            else:
                rows = pl.ds(way * (part // 2), part // 2)
                src = ow_ref.at[pl.ds(core * part + way * (part // 2), part // 2)] if r == 1 else ow_all.at[head, core, rows]
                send(src, ow_all.at[head, core, rows], ow_half, ow_sem.at[way, r - 1], {"tp": to})

    def ow_arrived(r):
        for way in range(2):
            head = lax.rem(tp + (r if way else -r) + tp_n, tp_n)
            if r < half_ring:
                landed(ow_all.at[head, core], ow_sem.at[way, r - 1])
            else:
                landed(ow_all.at[head, core, pl.ds(way * (part // 2), part // 2)], ow_sem.at[way, r - 1])
            if r < half_ring or way == 1:
                send(ow_all.at[head, core], ow_all.at[head, core], ow_sib_sent, ow_sib, at(chip, 1 - core))
        if r < half_ring:
            ow_stage(r + 1)

    def pass_on(k, src):
        place = kv_all.at[slot(core, own_g, k)]
        send(src, place, kv_sent, kv_fwd.at[k], at(beside))
        send(src, place, kv_sent, kv_sib.at[own_g, k], at(chip, 1 - core))

    pass_on(0, kv_ref.at[own_seq])
    ow_stage(1)
    for seq, g, home, k in homes:
        send(q_ref.at[seq], q_all.at[k], q_sent, q_sem.at[k], at(home))
    kv_all[own_slot] = kv_ref[own_seq]
    q_all[0] = q_ref[own_seq]
    ow_all[tp] = ow_ref[...].reshape(ow_all.shape[1:])

    low = lax.broadcasted_iota(jnp.int32, (half, LANES), 1) < LANES // 2
    factor = QK ** (-0.5) * math.log2(math.e)

    def attend(base, k, first, last):
        def rows(start):
            return kv_all[pl.ds(base, side), start : start + half, :].reshape(side * half, LANES)

        plain = q_all[k, :positions]
        first_rot = q_all[k, positions:].astype(jnp.float32)
        second_rot = pltpu.roll(first_rot, LANES // 2, 1)
        halves = [
            jnp.concatenate([jnp.where(low, first_rot, 0.0), jnp.where(low, second_rot, 0.0)], axis=0),
            jnp.concatenate([jnp.where(low, 0.0, second_rot), jnp.where(low, 0.0, first_rot)], axis=0),
        ]
        turned = rows(4 * half)
        scores = []
        for n in range(2):
            keys = jnp.concatenate([rows(n * half), turned], axis=1)
            q = jnp.concatenate([plain, halves[n].astype(jnp.bfloat16)], axis=1)
            scores.append(
                lax.dot_general(q, keys, (((1,), (1,)), ((), ())), preferred_element_type=jnp.float32)
            )
        top = jnp.maximum(jnp.max(scores[0], axis=1, keepdims=True), jnp.max(scores[1], axis=1, keepdims=True))
        if not first:
            old = run_max[k][:, :1]
            top = jnp.maximum(top, old)
            shrink = jnp.exp2((old - top) * factor)
        total, mixed = 0.0, 0.0
        for n in range(2):
            weights = jnp.exp2((scores[n] - top) * factor)
            total = total + jnp.sum(weights, axis=1, keepdims=True)
            mixed = mixed + jnp.dot(weights.astype(jnp.bfloat16), rows((2 + n) * half), preferred_element_type=jnp.float32)
        if not first:
            total = total + shrink * run_sum[k][:, :1]
            mixed = mixed + shrink * acc[k]
        if last:
            att[k] = (mixed / total).reshape(att.shape[1:]).astype(jnp.bfloat16)
        else:
            run_max[k] = jnp.broadcast_to(top, run_max.shape[1:])
            run_sum[k] = jnp.broadcast_to(total, run_sum.shape[1:])
            acc[k] = mixed

    def attend_all(base, first):
        def body(k, _):
            attend(base, k, first, False)
            return 0

        lax.fori_loop(0, side, body, 0)

    def direct_arrived(k):
        place = kv_all.at[slot(core, own_g, k)]
        landed(place, kv_sem.at[k])
        pass_on(k, place)

    def forward_arrived(k):
        place = kv_all.at[slot(core, 1 - own_g, k)]
        landed(place, kv_fwd.at[k])
        send(place, place, kv_sent, kv_sib.at[1 - own_g, k], at(chip, 1 - core))

    forward_arrived(0)
    for k in range(1, side):
        direct_arrived(k)
        if k == 1:
            ow_arrived(1)
        forward_arrived(k)
    for r in range(2, min(3, half_ring + 1)):
        ow_arrived(r)
    for k in range(1, side):
        landed(q_all.at[k], q_sem.at[k])
    attend_all(slot(core, own_g, 0), True)
    for k in range(side):
        landed(kv_all.at[slot(1 - core, own_g, k)], kv_sib.at[own_g, k])
    attend_all(slot(1 - core, own_g, 0), False)
    for r in range(3, half_ring):
        ow_arrived(r)
    attend_all(slot(core, 1 - own_g, 0), False)
    for k in range(side):
        landed(kv_all.at[slot(1 - core, 1 - own_g, k)], kv_sib.at[1 - own_g, k])
    for k in reversed(range(side)):
        attend(slot(1 - core, 1 - own_g, 0), k, False, True)
        if k > 0:
            send(att.at[k], heads_y.at[own_seq], y_sent, y_sem.at[own_seq], at(sources[k]))
    for e in range(seqs):
        seq, block = own_seq, att.at[0]
        if e > 0:
            seq = homes[e - 1][0]
            block = heads_y.at[seq]
            landed(block, y_sem.at[seq])
        for d in range(1, tp_n):
            to = lax.rem(tp + d, tp_n)
            send(block.at[to], heads_in.at[tp, seq], x_sent, x_sem, {"tp": to})
        heads_in[tp, seq] = block[tp]
    if half_ring > 2:
        ow_arrived(half_ring)
    landed(ow_all.at[pl.ds(0, tp_n - 1), 0], ow_sib)
    landed(heads_in.at[pl.ds(0, tp_n - 1)], x_sem)

    rows, width = res_ref.shape
    each = rows // seqs
    lhs = jnp.concatenate(
        [heads_in[h].astype(jnp.float32).reshape(rows, LANES).astype(jnp.bfloat16) for h in range(tp_n)], axis=1
    )
    r_out = lax.broadcasted_iota(jnp.int32, (rows, rows), 0)
    r_in = lax.broadcasted_iota(jnp.int32, (rows, rows), 1)
    shuffle = (r_in == lax.rem(r_out, seqs) * each + r_out // seqs).astype(jnp.float32).astype(jnp.bfloat16)
    lhs = jnp.dot(shuffle, lhs, preferred_element_type=jnp.float32).astype(jnp.bfloat16)
    squares = 0.0
    tile = 2 * LANES
    for j in range(width // tile):
        cols = slice(j * tile, (j + 1) * tile)
        weight = ow_all[:, :, :, cols].reshape(lhs.shape[1], tile)
        summed = res_ref[:, cols].astype(jnp.float32) + jnp.dot(lhs, weight, preferred_element_type=jnp.float32)
        rounded = summed.astype(jnp.bfloat16)
        stream_ref[:, cols] = rounded
        wide = rounded.astype(jnp.float32)
        squares = squares + jnp.sum(wide * wide, axis=1, keepdims=True)
    scale = lax.rsqrt(squares / width + epsilon)
    for j in range(width // tile):
        cols = slice(j * tile, (j + 1) * tile)
        normed_ref[:, cols] = (stream_ref[:, cols].astype(jnp.float32) * scale * gain_ref[:, cols]).astype(jnp.bfloat16)

    landed(kv_all.at[pl.ds(0, 4 * side - 1)], kv_sent)
    if seqs > 1:
        landed(q_all.at[pl.ds(0, seqs - 1)], q_sent)
        landed(att.at[pl.ds(0, side - 1)], y_sent)
    if half_ring > 1:
        landed(ow_all.at[pl.ds(0, 2 * (half_ring - 1)), 0], ow_sent)
    landed(ow_all.at[0, 0], ow_half)
    landed(ow_all.at[pl.ds(0, tp_n - 1), 0], ow_sib_sent)
    landed(heads_in.at[pl.ds(0, tp_n - 1)], x_sent)


def attention(sp_n, tp_n, queries, keyed, out_weight, residual, norm_gain):
    seqs, positions = queries.shape[0], queries.shape[1] // 3 * 2
    rows, width = residual.shape
    side = sp_n // 4
    each = positions // tp_n
    vmem = pl.BlockSpec(memory_space=pltpu.VMEM)
    dma = pltpu.SemaphoreType.DMA
    bf16, f32 = jnp.bfloat16, jnp.float32
    return pl.pallas_call(
        functools.partial(attention_kernel, sp_n, tp_n, seqs),
        out_shape=[jax.ShapeDtypeStruct((rows, width), bf16)] * 2,
        in_specs=[vmem] * 5,
        out_specs=[vmem] * 2,
        scratch_shapes=[
            pltpu.VMEM((4 * side,) + keyed.shape[1:], bf16),
            pltpu.VMEM((side,) + queries.shape[1:], bf16),
            pltpu.VMEM((tp_n, 2, out_weight.shape[0] // 2, width), bf16),
            pltpu.VMEM((side, tp_n, each, LANES), bf16),
            pltpu.VMEM((seqs, tp_n, each, LANES), bf16),
            pltpu.VMEM((tp_n, seqs, each, LANES), bf16),
            pltpu.VMEM((side, positions, LANES), f32),
            pltpu.VMEM((side, positions, LANES), f32),
            pltpu.VMEM((side, positions, LANES), f32),
            dma((side,)), dma((side,)), dma((2, side)), dma((side,)), dma((2, tp_n // 2)),
            dma, dma((seqs,)), dma, dma, dma, dma, dma, dma, dma, dma,
        ],
        compiler_params=pltpu.CompilerParams(collective_id=2, has_side_effects=True),
        name="attention",
    )(queries, keyed, out_weight, residual, norm_gain)


def prepared(query, latent, rope_key, latent_gain, key_up, value_up, own_positions):
    seqs = query.shape[1]
    half = query.shape[0] // 2
    by_seq = query.transpose(1, 0, 2)
    turned = rotate_by(by_seq[..., NOPE:].astype(jnp.float32), own_positions).astype(jnp.bfloat16)
    turned = jnp.concatenate([turned[:, :half], turned[:, half:]], axis=-1)
    queries = jnp.concatenate([by_seq[..., :NOPE], turned], axis=1)
    rows = latent.transpose(1, 0, 2)
    normed = rms_scale(rows.astype(jnp.float32), latent_gain).astype(jnp.bfloat16)
    keys = jnp.dot(normed, key_up, preferred_element_type=jnp.float32).astype(jnp.bfloat16)
    values = jnp.dot(normed, value_up, preferred_element_type=jnp.float32).astype(jnp.bfloat16)
    key_rot = rotate_by(rope_key.transpose(1, 0, 2).astype(jnp.float32), own_positions).astype(jnp.bfloat16)
    packed = jnp.concatenate([key_rot[:, :half], key_rot[:, half:]], axis=-1)
    return queries, jnp.concatenate([keys, values, packed], axis=1)


def moe_kernel(sp_n, tp_n, normed_ref, stream_ref, small_ref, wg_hbm, wu_hbm, wd_hbm, out_ref,
               wg, wu, wd, stage, rows_in, sums, w_sems, *scratch):
    chips = sp_n // 2
    peers = sp_n * tp_n
    plane = chips * tp_n
    rows, width = normed_ref.shape
    chunks = width // LANES
    span = CAP * chunks
    sp, tp = lax.axis_index("sp"), lax.axis_index("tp")
    chip, core = sp // 2, lax.rem(sp, 2)
    barrier = pltpu.get_barrier_semaphore()
    sibling = {"sp": 2 * chip + 1 - core}

    def across(d):
        to = lax.rem(tp + d, tp_n)
        return to, {"tp": to}

    def along(d):
        to = lax.rem(chip + d, chips)
        return to, {"sp": 2 * to + core}

    ring = []
    for d in reversed(range(1, max(chips, tp_n) // 2 + 1)):
        for step in (d, -d):
            if d < tp_n and (step > 0 or 2 * d != tp_n) and d <= tp_n // 2:
                ring.append((across, step % tp_n))
            if d < chips and (step > 0 or 2 * d != chips) and d <= chips // 2:
                ring.append((along, step % chips))
    for where in [sibling] + [way(d)[1] for way, d in ring]:
        pl.semaphore_signal(barrier, inc=1, device_id=where, device_id_type=MESH)
    loads = [
        pltpu.make_async_copy(src, dst, w_sems.at[k])
        for k, (src, dst) in enumerate(((wg_hbm, wg), (wu_hbm, wu), (wd_hbm, wd)))
    ]
    for load in loads:
        load.start()

    def send(src, dst, sent, got, where):
        pltpu.make_async_remote_copy(
            src_ref=src, dst_ref=dst, send_sem=sent, recv_sem=got, device_id=where, device_id_type=MESH
        ).start()

    def landed(buffer, sem):
        pltpu.make_async_copy(buffer, buffer, sem).wait()

    def part(p):
        return pl.ds(p * chunks, chunks)

    def begin(buffers, p):
        held, given, by_tp, by_sp, from_even, from_odd, sems, swap = buffers
        send(given.at[:, part(p)], held.at[core, :, part(p)], swap.at[p, 0], swap.at[p, 1], sibling)
        pl.when(core == 0)(functools.partial(even_first, buffers, p))
        pl.when(core == 1)(functools.partial(odd_first, buffers, p))

    def even_first(buffers, p):
        held, given, by_tp, by_sp, from_even, from_odd, sems, swap = buffers
        for way, d in ring:
            if way is across:
                to, where = across(d)
                src = held.at[0, pl.ds(to * chips, chips), part(p)]
                send(src, by_tp.at[tp, :, part(p)], sems.at[p, 0], sems.at[p, 1], where)

    def odd_first(buffers, p):
        held, given, by_tp, by_sp, from_even, from_odd, sems, swap = buffers
        for way, d in ring:
            if way is along:
                to, where = along(d)
                src = held.at[1, pl.ds(to * tp_n, tp_n), part(p)]
                send(src, by_sp.at[chip, :, part(p)], sems.at[p, 2], sems.at[p, 3], where)

    def rest(buffers, p):
        held, given, by_tp, by_sp, from_even, from_odd, sems, swap = buffers
        landed(given.at[:, part(p)], swap.at[p, 1])
        pl.when(core == 1)(functools.partial(even_first, buffers, p))
        pl.when(core == 0)(functools.partial(odd_first, buffers, p))
        by_tp[tp, :, part(p)] = held[0, pl.ds(tp * chips, chips), part(p)]
        by_sp[chip, :, part(p)] = held[1, pl.ds(chip * tp_n, tp_n), part(p)]

    def turn(buffers, p):
        held, given, by_tp, by_sp, from_even, from_odd, sems, swap = buffers
        landed(by_tp.at[pl.ds(0, tp_n - 1), :, part(p)], sems.at[p, 1])
        for way, d in ring:
            if way is along:
                to, where = along(d)
                send(by_tp.at[:, to, part(p)], from_even.at[chip, :, part(p)], sems.at[p, 4], sems.at[p, 5], where)
        landed(by_sp.at[pl.ds(0, chips - 1), :, part(p)], sems.at[p, 3])
        for way, d in ring:
            if way is across:
                to, where = across(d)
                send(by_sp.at[:, to, part(p)], from_odd.at[tp, :, part(p)], sems.at[p, 6], sems.at[p, 7], where)
        from_even[chip, :, part(p)] = by_tp[:, chip, part(p)]
        from_odd[tp, :, part(p)] = by_sp[:, tp, part(p)]

    def finish(buffers, p):
        held, given, by_tp, by_sp, from_even, from_odd, sems, swap = buffers
        landed(from_even.at[pl.ds(0, chips - 1), :, part(p)], sems.at[p, 5])
        landed(from_odd.at[pl.ds(0, tp_n - 1), :, part(p)], sems.at[p, 7])

    def sent(buffers):
        held, given, by_tp, by_sp, from_even, from_odd, sems, swap = buffers
        for p in range(CAP):
            landed(given.at[:, part(p)], swap.at[p, 0])
            landed(by_tp.at[pl.ds(0, tp_n - 1), :, part(p)], sems.at[p, 0])
            landed(by_sp.at[pl.ds(0, chips - 1), :, part(p)], sems.at[p, 2])
            landed(from_even.at[pl.ds(0, chips - 1), :, part(p)], sems.at[p, 4])
            landed(from_odd.at[pl.ds(0, tp_n - 1), :, part(p)], sems.at[p, 6])

    def device(c, core_id, x):
        return (2 * c + core_id) * tp_n + x

    step = min(8, plane)

    def pack(buffers, p):
        held, given = buffers[:2]

        def block(i, to_core):
            c = lax.rem(i, chips) * (1 - core) + i // tp_n * core
            x = i // chips * (1 - core) + lax.rem(i, tp_n) * core
            start = pl.multiple_of(device(c, to_core, x) * span, span) + p * chunks
            return stage[pl.ds(start, chunks), :].astype(jnp.bfloat16)

        def body(n, _):
            for j in range(step):
                i = n * step + j
                held[core, i, part(p)] = block(i, core)
                given[i, part(p)] = block(i, 1 - core)
            return 0

        lax.fori_loop(0, plane // step, body, 0)

    def unpack(buffers, p):
        from_even, from_odd = buffers[4:6]

        def put(where, block):
            start = pl.multiple_of(where * span, span) + p * chunks
            stage[pl.ds(start, chunks), :] = block.astype(jnp.float32)

        def body(n, _):
            for j in range(step):
                i = n * step + j
                c, x = i // tp_n, lax.rem(i, tp_n)
                put(device(c, 0, x), from_even[c, x, part(p)])
                put(device(c, 1, x), from_odd[x, c, part(p)])
            return 0

        lax.fori_loop(0, plane // step, body, 0)

    experts = lax.broadcasted_iota(jnp.int32, (rows, peers), 1).astype(jnp.float32)
    small = small_ref[...]
    picks = [(small[:, k : k + 1] == experts).astype(jnp.float32) for k in range(TOPK)]
    logits = [small[:, TOPK + k : TOPK + k + 1] for k in range(TOPK)]
    top = jnp.maximum(logits[0], logits[1])
    raised = [jnp.exp(v - top) for v in logits]
    shared = small[:, 2 * TOPK : 2 * TOPK + 1]
    mixing = [v / (raised[0] + raised[1]) * shared for v in raised]
    both = (picks[0] + picks[1]).astype(jnp.bfloat16)
    earlier = (
        lax.broadcasted_iota(jnp.int32, (rows, rows), 0) > lax.broadcasted_iota(jnp.int32, (rows, rows), 1)
    ).astype(jnp.float32).astype(jnp.bfloat16)
    before = jnp.dot(earlier, both, preferred_element_type=jnp.float32)
    chosen = []
    for pick in picks:
        slot = jnp.sum(pick * before, axis=1, keepdims=True)
        chosen.append(jnp.concatenate([pick * (1.0 - slot), pick * slot], axis=1))
    taken = (chosen[0] + chosen[1]).astype(jnp.bfloat16)
    chosen = [c.astype(jnp.bfloat16) for c in chosen]

    for j in range(chunks // 2):
        placed = lax.dot_general(
            taken, normed_ref[:, 2 * j * LANES : (2 * j + 2) * LANES], (((0,), (0,)), ((), ())),
            preferred_element_type=jnp.float32,
        )
        for c in range(CAP):
            for h in range(2):
                stage[pl.ds(c * chunks + 2 * j + h, peers, stride=span), :] = placed[
                    c * peers : (c + 1) * peers, h * LANES : (h + 1) * LANES
                ]
    there, back = scratch[:8], scratch[8:]
    for p in range(CAP):
        pack(there, p)
    pl.semaphore_wait(barrier, len(ring) + 1)
    for p in range(CAP):
        begin(there, p)
    for p in range(CAP):
        rest(there, p)
    for p in range(CAP):
        turn(there, p)
    for load in loads:
        load.wait()

    tile = 256

    def serve(p):
        for l in range(chunks):
            rows_in[:, l * LANES : (l + 1) * LANES] = stage[pl.ds(p * chunks + l, peers, stride=span), :].astype(
                jnp.bfloat16
            )
        hidden = []
        for j in range(wg.shape[1] // tile):
            cols = slice(j * tile, (j + 1) * tile)
            gate = jnp.dot(rows_in[...], wg[:, cols], preferred_element_type=jnp.float32)
            up = jnp.dot(rows_in[...], wu[:, cols], preferred_element_type=jnp.float32)
            hidden.append((gate / (1.0 + jnp.exp(-gate)) * up).astype(jnp.bfloat16))
        hidden = jnp.concatenate(hidden, axis=1)
        for j in range(chunks // 2):
            out = jnp.dot(hidden, wd[:, 2 * j * LANES : (2 * j + 2) * LANES], preferred_element_type=jnp.float32)
            for h in range(2):
                stage[pl.ds(p * chunks + 2 * j + h, peers, stride=span), :] = out[:, h * LANES : (h + 1) * LANES]

    for p in range(CAP):
        finish(there, p)
        unpack(there, p)
        serve(p)
        pack(back, p)
        begin(back, p)
        rest(back, p)
    for p in range(CAP):
        turn(back, p)

    for p in range(CAP):
        finish(back, p)
        unpack(back, p)
        for j in range(chunks // 2):
            block = jnp.concatenate(
                [stage[pl.ds(p * chunks + 2 * j + h, peers, stride=span), :] for h in range(2)], axis=1
            ).astype(jnp.bfloat16)
            cols = slice(2 * j * LANES, (2 * j + 2) * LANES)
            added = 0.0 if p == 0 else sums[:, cols]
            for k in range(TOPK):
                picked = chosen[k][:, p * peers : (p + 1) * peers]
                added = added + mixing[k] * jnp.dot(picked, block, preferred_element_type=jnp.float32)
            if p < CAP - 1:
                sums[:, cols] = added
            else:
                out_ref[:, cols] = (stream_ref[:, cols].astype(jnp.float32) + added).astype(jnp.bfloat16)
    sent(there)
    sent(back)


def routed_experts(sp_n, tp_n, normed, stream, small, w_gate, w_up, w_down):
    rows, width = normed.shape
    peers = sp_n * tp_n
    chips = sp_n // 2
    span = CAP * width // LANES
    vmem = pl.BlockSpec(memory_space=pltpu.VMEM)
    hbm = pl.BlockSpec(memory_space=pl.ANY)
    dma = pltpu.SemaphoreType.DMA

    def blocks(*lead):
        return pltpu.VMEM((*lead, span, LANES), jnp.bfloat16)

    buffers = [
        blocks(2, chips * tp_n), blocks(chips * tp_n), blocks(tp_n, chips), blocks(chips, tp_n), blocks(chips, tp_n),
        blocks(tp_n, chips), dma((CAP, 8)), dma((CAP, 2)),
    ]
    return pl.pallas_call(
        functools.partial(moe_kernel, sp_n, tp_n),
        out_shape=jax.ShapeDtypeStruct((rows, width), jnp.bfloat16),
        in_specs=[vmem] * 3 + [hbm] * 3,
        out_specs=vmem,
        scratch_shapes=[
            pltpu.VMEM(w_gate.shape, jnp.bfloat16),
            pltpu.VMEM(w_up.shape, jnp.bfloat16),
            pltpu.VMEM(w_down.shape, jnp.bfloat16),
            pltpu.VMEM((peers * span, LANES), jnp.float32),
            pltpu.VMEM((peers, width), jnp.bfloat16),
            pltpu.VMEM((rows, width), jnp.float32),
            dma((3,)),
            *buffers,
            *buffers,
        ],
        compiler_params=pltpu.CompilerParams(collective_id=1, has_side_effects=True),
        name="routed_experts",
    )(normed, stream, small, w_gate, w_up, w_down)


def shards(
    residual,
    query,
    latent,
    rope_key,
    latent_gain,
    key_up,
    value_up,
    out_weight,
    norm_gain,
    group_prob,
    pair_logits,
    routes,
    w_gate,
    w_up,
    w_down,
):
    positions_here = query.shape[0]
    own_positions = lax.axis_index("sp") * positions_here + jnp.arange(
        positions_here, dtype=jnp.int32
    )
    row_count = residual.shape[0] * residual.shape[1]
    queries, keyed = prepared(query, latent, rope_key, latent_gain, key_up, value_up, own_positions)
    stream, normed = attention(
        lax.axis_size("sp"),
        lax.axis_size("tp"),
        queries,
        keyed,
        out_weight,
        residual.reshape(row_count, D),
        norm_gain.reshape(1, D),
    )
    small = jnp.concatenate([routes.astype(jnp.float32), pair_logits, group_prob[..., None]], axis=-1)
    combined = routed_experts(
        lax.axis_size("sp"),
        lax.axis_size("tp"),
        normed,
        stream,
        small.reshape(row_count, 2 * TOPK + 1),
        w_gate[0],
        w_up[0],
        w_down[0],
    )
    return combined.reshape(residual.shape)


def solution(mesh):
    placed = (
        P(("sp", "tp"), "grp", None),
        P("sp", "grp", "tp"),
        P("sp", "grp", None),
        P("sp", "grp", None),
        P(),
        P(None, "tp"),
        P(None, "tp"),
        P("tp", None),
        P(),
        P(("sp", "tp"), "grp"),
        P(("sp", "tp"), "grp", None),
        P(("sp", "tp"), "grp", None),
        P(("sp", "tp"), None, None),
        P(("sp", "tp"), None, None),
        P(("sp", "tp"), None, None),
    )
    return jax.shard_map(
        shards, mesh=mesh, in_specs=placed, out_specs=P(("sp", "tp"), "grp", None), check_vma=False
    )
```

```python
import functools
import math

import jax
import jax.numpy as jnp
from jax import lax
from jax.experimental import pallas as pl
from jax.experimental.pallas import tpu as pltpu
from jax.sharding import PartitionSpec as P

D = 2048
NOPE = 128
QK = 192
TOPK = 2
CAP = 2
LANES = 128
MESH = pl.DeviceIdType.MESH


epsilon = 1e-06
rotary_base = 10000.0


def rotate_by(values, positions):
    halfway = values.shape[-1] // 2
    inverse = rotary_base ** (-jnp.arange(halfway, dtype=jnp.float32) / halfway)
    angles = positions.astype(jnp.float32)[:, None] * inverse[None, :]
    cosine_values = jnp.cos(angles)
    sine_values = jnp.sin(angles)
    first_half = values[..., :halfway]
    second_half = values[..., halfway:]
    return jnp.concatenate(
        [
            first_half * cosine_values - second_half * sine_values,
            second_half * cosine_values + first_half * sine_values,
        ],
        axis=-1,
    )


def rms_scale(values, gain_values):
    return (
        values
        * lax.rsqrt(jnp.mean(values * values, axis=-1, keepdims=True) + epsilon)
        * gain_values
    )


def attention_kernel(sp_n, tp_n, seqs, q_ref, kv_ref, ow_ref, res_ref, gain_ref, stream_ref, normed_ref,
                     kv_all, q_all, ow_all, att, heads_y, heads_in, run_max, run_sum, acc,
                     kv_sem, kv_fwd, kv_sib, q_sem, ow_sem, ow_sib, y_sem, x_sem, kv_sent, q_sent, ow_sent, ow_half, ow_sib_sent, y_sent, x_sent):
    chips = sp_n // 2
    side = chips // 2
    half_ring = tp_n // 2
    sp, tp = lax.axis_index("sp"), lax.axis_index("tp")
    chip, core = sp // 2, lax.rem(sp, 2)
    own_seq, own_g = chip // 2, lax.rem(chip, 2)
    half = q_ref.shape[1] // 3
    positions = 2 * half
    part = ow_ref.shape[0] // 2

    def at(chip_id, core_id=None):
        return {"sp": 2 * chip_id + (core if core_id is None else core_id)}

    homes = []
    for e in range(1, seqs):
        seq = lax.rem(own_seq + e, seqs)
        delta = lax.rem(chip - 2 * seq + chips, chips)
        g = 1 - lax.rem(delta + chips - 1, chips) // side
        home = 2 * seq + g
        k = g * lax.rem(chip - home + chips, chips) + (1 - g) * lax.rem(home - chip + chips, chips)
        homes.append((seq, g, home, k))
    sources = [lax.rem(chip + (2 * own_g - 1) * k + chips, chips) for k in range(side)]
    beside = 2 * own_seq + 1 - own_g
    right, left = lax.rem(tp + 1, tp_n), lax.rem(tp + tp_n - 1, tp_n)

    def slot(core_id, g, k):
        return (core_id * 2 + g) * side + k

    def send(src, dst, sent, got, where):
        pltpu.make_async_remote_copy(
            src_ref=src, dst_ref=dst, send_sem=sent, recv_sem=got, device_id=where, device_id_type=MESH
        ).start()

    def landed(buffer, sem):
        pltpu.make_async_copy(buffer, buffer, sem).wait()

    barrier = pltpu.get_barrier_semaphore()
    peers = [at(h[2]) for h in homes] + [at(s) for s in sources[1:]] + [at(beside), at(chip, 1 - core)]
    peers += [{"tp": lax.rem(tp + d, tp_n)} for d in range(1, tp_n)]
    for where in peers:
        pl.semaphore_signal(barrier, inc=1, device_id=where, device_id_type=MESH)
    pl.semaphore_wait(barrier, len(peers))

    own_slot = slot(core, own_g, 0)
    for seq, g, home, k in homes[1:2] + homes[:1] + homes[2:]:
        send(kv_ref.at[seq], kv_all.at[slot(core, g, k)], kv_sent, kv_sem.at[k], at(home))

    def ow_stage(r):
        for way, to in ((0, right), (1, left)):
            head = lax.rem(tp + (r - 1 if way else 1 - r) + tp_n, tp_n)
            if r < half_ring:
                src = ow_ref.at[pl.ds(core * part, part)] if r == 1 else ow_all.at[head, core]
                send(src, ow_all.at[head, core], ow_sent, ow_sem.at[way, r - 1], {"tp": to})
            else:
                rows = pl.ds(way * (part // 2), part // 2)
                src = ow_ref.at[pl.ds(core * part + way * (part // 2), part // 2)] if r == 1 else ow_all.at[head, core, rows]
                send(src, ow_all.at[head, core, rows], ow_half, ow_sem.at[way, r - 1], {"tp": to})

    def ow_arrived(r):
        for way in range(2):
            head = lax.rem(tp + (r if way else -r) + tp_n, tp_n)
            if r < half_ring:
                landed(ow_all.at[head, core], ow_sem.at[way, r - 1])
            else:
                landed(ow_all.at[head, core, pl.ds(way * (part // 2), part // 2)], ow_sem.at[way, r - 1])
            if r < half_ring or way == 1:
                send(ow_all.at[head, core], ow_all.at[head, core], ow_sib_sent, ow_sib, at(chip, 1 - core))
        if r < half_ring:
            ow_stage(r + 1)

    def pass_on(k, src):
        place = kv_all.at[slot(core, own_g, k)]
        send(src, place, kv_sent, kv_fwd.at[k], at(beside))
        send(src, place, kv_sent, kv_sib.at[own_g, k], at(chip, 1 - core))

    pass_on(0, kv_ref.at[own_seq])
    ow_stage(1)
    for seq, g, home, k in homes:
        send(q_ref.at[seq], q_all.at[k], q_sent, q_sem.at[k], at(home))
    kv_all[own_slot] = kv_ref[own_seq]
    q_all[0] = q_ref[own_seq]
    ow_all[tp] = ow_ref[...].reshape(ow_all.shape[1:])

    low = lax.broadcasted_iota(jnp.int32, (half, LANES), 1) < LANES // 2
    factor = QK ** (-0.5) * math.log2(math.e)

    def attend(base, k, first, last):
        def rows(start):
            return kv_all[pl.ds(base, side), start : start + half, :].reshape(side * half, LANES)

        plain = q_all[k, :positions]
        first_rot = q_all[k, positions:].astype(jnp.float32)
        second_rot = pltpu.roll(first_rot, LANES // 2, 1)
        halves = [
            jnp.concatenate([jnp.where(low, first_rot, 0.0), jnp.where(low, second_rot, 0.0)], axis=0),
            jnp.concatenate([jnp.where(low, 0.0, second_rot), jnp.where(low, 0.0, first_rot)], axis=0),
        ]
        turned = rows(4 * half)
        scores = []
        for n in range(2):
            keys = jnp.concatenate([rows(n * half), turned], axis=1)
            q = jnp.concatenate([plain, halves[n].astype(jnp.bfloat16)], axis=1)
            scores.append(
                lax.dot_general(q, keys, (((1,), (1,)), ((), ())), preferred_element_type=jnp.float32)
            )
        top = jnp.maximum(jnp.max(scores[0], axis=1, keepdims=True), jnp.max(scores[1], axis=1, keepdims=True))
        if not first:
            old = run_max[k][:, :1]
            top = jnp.maximum(top, old)
            shrink = jnp.exp2((old - top) * factor)
        total, mixed = 0.0, 0.0
        for n in range(2):
            weights = jnp.exp2((scores[n] - top) * factor)
            total = total + jnp.sum(weights, axis=1, keepdims=True)
            mixed = mixed + jnp.dot(weights.astype(jnp.bfloat16), rows((2 + n) * half), preferred_element_type=jnp.float32)
        if not first:
            total = total + shrink * run_sum[k][:, :1]
            mixed = mixed + shrink * acc[k]
        if last:
            att[k] = (mixed / total).reshape(att.shape[1:]).astype(jnp.bfloat16)
        else:
            run_max[k] = jnp.broadcast_to(top, run_max.shape[1:])
            run_sum[k] = jnp.broadcast_to(total, run_sum.shape[1:])
            acc[k] = mixed

    def attend_all(base, first):
        def body(k, _):
            attend(base, k, first, False)
            return 0

        lax.fori_loop(0, side, body, 0)

    def direct_arrived(k):
        place = kv_all.at[slot(core, own_g, k)]
        landed(place, kv_sem.at[k])
        pass_on(k, place)

    def forward_arrived(k):
        place = kv_all.at[slot(core, 1 - own_g, k)]
        landed(place, kv_fwd.at[k])
        send(place, place, kv_sent, kv_sib.at[1 - own_g, k], at(chip, 1 - core))

    forward_arrived(0)
    for k in range(1, side):
        direct_arrived(k)
        if k == 1:
            ow_arrived(1)
        forward_arrived(k)
    for r in range(2, min(3, half_ring + 1)):
        ow_arrived(r)
    for k in range(1, side):
        landed(q_all.at[k], q_sem.at[k])
    attend_all(slot(core, own_g, 0), True)
    for k in range(side):
        landed(kv_all.at[slot(1 - core, own_g, k)], kv_sib.at[own_g, k])
    attend_all(slot(1 - core, own_g, 0), False)
    for r in range(3, half_ring):
        ow_arrived(r)
    attend_all(slot(core, 1 - own_g, 0), False)
    for k in range(side):
        landed(kv_all.at[slot(1 - core, 1 - own_g, k)], kv_sib.at[1 - own_g, k])
    for k in reversed(range(side)):
        attend(slot(1 - core, 1 - own_g, 0), k, False, True)
        if k > 0:
            send(att.at[k], heads_y.at[own_seq], y_sent, y_sem.at[own_seq], at(sources[k]))
    for e in range(seqs):
        seq, block = own_seq, att.at[0]
        if e > 0:
            seq = homes[e - 1][0]
            block = heads_y.at[seq]
            landed(block, y_sem.at[seq])
        for d in range(1, tp_n):
            to = lax.rem(tp + d, tp_n)
            send(block.at[to], heads_in.at[tp, seq], x_sent, x_sem, {"tp": to})
        heads_in[tp, seq] = block[tp]
    if half_ring > 2:
        ow_arrived(half_ring)
    landed(ow_all.at[pl.ds(0, tp_n - 1), 0], ow_sib)
    landed(heads_in.at[pl.ds(0, tp_n - 1)], x_sem)

    rows, width = res_ref.shape
    each = rows // seqs
    lhs = jnp.concatenate(
        [heads_in[h].astype(jnp.float32).reshape(rows, LANES).astype(jnp.bfloat16) for h in range(tp_n)], axis=1
    )
    r_out = lax.broadcasted_iota(jnp.int32, (rows, rows), 0)
    r_in = lax.broadcasted_iota(jnp.int32, (rows, rows), 1)
    shuffle = (r_in == lax.rem(r_out, seqs) * each + r_out // seqs).astype(jnp.float32).astype(jnp.bfloat16)
    lhs = jnp.dot(shuffle, lhs, preferred_element_type=jnp.float32).astype(jnp.bfloat16)
    squares = 0.0
    tile = 2 * LANES
    for j in range(width // tile):
        cols = slice(j * tile, (j + 1) * tile)
        weight = ow_all[:, :, :, cols].reshape(lhs.shape[1], tile)
        summed = res_ref[:, cols].astype(jnp.float32) + jnp.dot(lhs, weight, preferred_element_type=jnp.float32)
        rounded = summed.astype(jnp.bfloat16)
        stream_ref[:, cols] = rounded
        wide = rounded.astype(jnp.float32)
        squares = squares + jnp.sum(wide * wide, axis=1, keepdims=True)
    scale = lax.rsqrt(squares / width + epsilon)
    for j in range(width // tile):
        cols = slice(j * tile, (j + 1) * tile)
        normed_ref[:, cols] = (stream_ref[:, cols].astype(jnp.float32) * scale * gain_ref[:, cols]).astype(jnp.bfloat16)

    landed(kv_all.at[pl.ds(0, 4 * side - 1)], kv_sent)
    if seqs > 1:
        landed(q_all.at[pl.ds(0, seqs - 1)], q_sent)
        landed(att.at[pl.ds(0, side - 1)], y_sent)
    if half_ring > 1:
        landed(ow_all.at[pl.ds(0, 2 * (half_ring - 1)), 0], ow_sent)
    landed(ow_all.at[0, 0], ow_half)
    landed(ow_all.at[pl.ds(0, tp_n - 1), 0], ow_sib_sent)
    landed(heads_in.at[pl.ds(0, tp_n - 1)], x_sent)


def attention(sp_n, tp_n, queries, keyed, out_weight, residual, norm_gain):
    seqs, positions = queries.shape[0], queries.shape[1] // 3 * 2
    rows, width = residual.shape
    side = sp_n // 4
    each = positions // tp_n
    vmem = pl.BlockSpec(memory_space=pltpu.VMEM)
    dma = pltpu.SemaphoreType.DMA
    bf16, f32 = jnp.bfloat16, jnp.float32
    return pl.pallas_call(
        functools.partial(attention_kernel, sp_n, tp_n, seqs),
        out_shape=[jax.ShapeDtypeStruct((rows, width), bf16)] * 2,
        in_specs=[vmem] * 5,
        out_specs=[vmem] * 2,
        scratch_shapes=[
            pltpu.VMEM((4 * side,) + keyed.shape[1:], bf16),
            pltpu.VMEM((side,) + queries.shape[1:], bf16),
            pltpu.VMEM((tp_n, 2, out_weight.shape[0] // 2, width), bf16),
            pltpu.VMEM((side, tp_n, each, LANES), bf16),
            pltpu.VMEM((seqs, tp_n, each, LANES), bf16),
            pltpu.VMEM((tp_n, seqs, each, LANES), bf16),
            pltpu.VMEM((side, positions, LANES), f32),
            pltpu.VMEM((side, positions, LANES), f32),
            pltpu.VMEM((side, positions, LANES), f32),
            dma((side,)), dma((side,)), dma((2, side)), dma((side,)), dma((2, tp_n // 2)),
            dma, dma((seqs,)), dma, dma, dma, dma, dma, dma, dma, dma,
        ],
        compiler_params=pltpu.CompilerParams(collective_id=2, has_side_effects=True),
        name="attention",
    )(queries, keyed, out_weight, residual, norm_gain)


def prepared(query, latent, rope_key, latent_gain, key_up, value_up, own_positions):
    seqs = query.shape[1]
    half = query.shape[0] // 2
    by_seq = query.transpose(1, 0, 2)
    turned = rotate_by(by_seq[..., NOPE:].astype(jnp.float32), own_positions).astype(jnp.bfloat16)
    turned = jnp.concatenate([turned[:, :half], turned[:, half:]], axis=-1)
    queries = jnp.concatenate([by_seq[..., :NOPE], turned], axis=1)
    rows = latent.transpose(1, 0, 2)
    normed = rms_scale(rows.astype(jnp.float32), latent_gain).astype(jnp.bfloat16)
    keys = jnp.dot(normed, key_up, preferred_element_type=jnp.float32).astype(jnp.bfloat16)
    values = jnp.dot(normed, value_up, preferred_element_type=jnp.float32).astype(jnp.bfloat16)
    key_rot = rotate_by(rope_key.transpose(1, 0, 2).astype(jnp.float32), own_positions).astype(jnp.bfloat16)
    packed = jnp.concatenate([key_rot[:, :half], key_rot[:, half:]], axis=-1)
    return queries, jnp.concatenate([keys, values, packed], axis=1)


def moe_kernel(sp_n, tp_n, normed_ref, stream_ref, small_ref, wg_hbm, wu_hbm, wd_hbm, out_ref,
               wg, wu, wd, stage, rows_in, sums, w_sems, *scratch):
    chips = sp_n // 2
    peers = sp_n * tp_n
    plane = chips * tp_n
    rows, width = normed_ref.shape
    chunks = width // LANES
    span = CAP * chunks
    sp, tp = lax.axis_index("sp"), lax.axis_index("tp")
    chip, core = sp // 2, lax.rem(sp, 2)
    barrier = pltpu.get_barrier_semaphore()
    sibling = {"sp": 2 * chip + 1 - core}

    def across(d):
        to = lax.rem(tp + d, tp_n)
        return to, {"tp": to}

    def along(d):
        to = lax.rem(chip + d, chips)
        return to, {"sp": 2 * to + core}

    ring = []
    for d in reversed(range(1, max(chips, tp_n) // 2 + 1)):
        for step in (d, -d):
            if d < tp_n and (step > 0 or 2 * d != tp_n) and d <= tp_n // 2:
                ring.append((across, step % tp_n))
            if d < chips and (step > 0 or 2 * d != chips) and d <= chips // 2:
                ring.append((along, step % chips))
    for where in [sibling] + [way(d)[1] for way, d in ring]:
        pl.semaphore_signal(barrier, inc=1, device_id=where, device_id_type=MESH)
    loads = [
        pltpu.make_async_copy(src, dst, w_sems.at[k])
        for k, (src, dst) in enumerate(((wg_hbm, wg), (wu_hbm, wu), (wd_hbm, wd)))
    ]
    for load in loads:
        load.start()

    def send(src, dst, sent, got, where):
        pltpu.make_async_remote_copy(
            src_ref=src, dst_ref=dst, send_sem=sent, recv_sem=got, device_id=where, device_id_type=MESH
        ).start()

    def landed(buffer, sem):
        pltpu.make_async_copy(buffer, buffer, sem).wait()

    def part(p):
        return pl.ds(p * chunks, chunks)

    def begin(buffers, p):
        held, given, by_tp, by_sp, from_even, from_odd, sems, swap = buffers
        send(given.at[:, part(p)], held.at[core, :, part(p)], swap.at[p, 0], swap.at[p, 1], sibling)
        pl.when(core == 0)(functools.partial(even_first, buffers, p))
        pl.when(core == 1)(functools.partial(odd_first, buffers, p))

    def even_first(buffers, p):
        held, given, by_tp, by_sp, from_even, from_odd, sems, swap = buffers
        for way, d in ring:
            if way is across:
                to, where = across(d)
                src = held.at[0, pl.ds(to * chips, chips), part(p)]
                send(src, by_tp.at[tp, :, part(p)], sems.at[p, 0], sems.at[p, 1], where)

    def odd_first(buffers, p):
        held, given, by_tp, by_sp, from_even, from_odd, sems, swap = buffers
        for way, d in ring:
            if way is along:
                to, where = along(d)
                src = held.at[1, pl.ds(to * tp_n, tp_n), part(p)]
                send(src, by_sp.at[chip, :, part(p)], sems.at[p, 2], sems.at[p, 3], where)

    def rest(buffers, p):
        held, given, by_tp, by_sp, from_even, from_odd, sems, swap = buffers
        landed(given.at[:, part(p)], swap.at[p, 1])
        pl.when(core == 1)(functools.partial(even_first, buffers, p))
        pl.when(core == 0)(functools.partial(odd_first, buffers, p))
        by_tp[tp, :, part(p)] = held[0, pl.ds(tp * chips, chips), part(p)]
        by_sp[chip, :, part(p)] = held[1, pl.ds(chip * tp_n, tp_n), part(p)]

    def turn(buffers, p):
        held, given, by_tp, by_sp, from_even, from_odd, sems, swap = buffers
        landed(by_tp.at[pl.ds(0, tp_n - 1), :, part(p)], sems.at[p, 1])
        for way, d in ring:
            if way is along:
                to, where = along(d)
                send(by_tp.at[:, to, part(p)], from_even.at[chip, :, part(p)], sems.at[p, 4], sems.at[p, 5], where)
        landed(by_sp.at[pl.ds(0, chips - 1), :, part(p)], sems.at[p, 3])
        for way, d in ring:
            if way is across:
                to, where = across(d)
                send(by_sp.at[:, to, part(p)], from_odd.at[tp, :, part(p)], sems.at[p, 6], sems.at[p, 7], where)
        from_even[chip, :, part(p)] = by_tp[:, chip, part(p)]
        from_odd[tp, :, part(p)] = by_sp[:, tp, part(p)]

    def finish(buffers, p):
        held, given, by_tp, by_sp, from_even, from_odd, sems, swap = buffers
        landed(from_even.at[pl.ds(0, chips - 1), :, part(p)], sems.at[p, 5])
        landed(from_odd.at[pl.ds(0, tp_n - 1), :, part(p)], sems.at[p, 7])

    def sent(buffers):
        held, given, by_tp, by_sp, from_even, from_odd, sems, swap = buffers
        for p in range(CAP):
            landed(given.at[:, part(p)], swap.at[p, 0])
            landed(by_tp.at[pl.ds(0, tp_n - 1), :, part(p)], sems.at[p, 0])
            landed(by_sp.at[pl.ds(0, chips - 1), :, part(p)], sems.at[p, 2])
            landed(from_even.at[pl.ds(0, chips - 1), :, part(p)], sems.at[p, 4])
            landed(from_odd.at[pl.ds(0, tp_n - 1), :, part(p)], sems.at[p, 6])

    def device(c, core_id, x):
        return (2 * c + core_id) * tp_n + x

    step = min(8, plane)

    def pack(buffers, p):
        held, given = buffers[:2]

        def block(i, to_core):
            c = lax.rem(i, chips) * (1 - core) + i // tp_n * core
            x = i // chips * (1 - core) + lax.rem(i, tp_n) * core
            start = pl.multiple_of(device(c, to_core, x) * span, span) + p * chunks
            return stage[pl.ds(start, chunks), :].astype(jnp.bfloat16)

        def body(n, _):
            for j in range(step):
                i = n * step + j
                held[core, i, part(p)] = block(i, core)
                given[i, part(p)] = block(i, 1 - core)
            return 0

        lax.fori_loop(0, plane // step, body, 0)

    def unpack(buffers, p):
        from_even, from_odd = buffers[4:6]

        def put(where, block):
            start = pl.multiple_of(where * span, span) + p * chunks
            stage[pl.ds(start, chunks), :] = block.astype(jnp.float32)

        def body(n, _):
            for j in range(step):
                i = n * step + j
                c, x = i // tp_n, lax.rem(i, tp_n)
                put(device(c, 0, x), from_even[c, x, part(p)])
                put(device(c, 1, x), from_odd[x, c, part(p)])
            return 0

        lax.fori_loop(0, plane // step, body, 0)

    experts = lax.broadcasted_iota(jnp.int32, (rows, peers), 1).astype(jnp.float32)
    small = small_ref[...]
    picks = [(small[:, k : k + 1] == experts).astype(jnp.float32) for k in range(TOPK)]
    logits = [small[:, TOPK + k : TOPK + k + 1] for k in range(TOPK)]
    top = jnp.maximum(logits[0], logits[1])
    raised = [jnp.exp(v - top) for v in logits]
    shared = small[:, 2 * TOPK : 2 * TOPK + 1]
    mixing = [v / (raised[0] + raised[1]) * shared for v in raised]
    both = (picks[0] + picks[1]).astype(jnp.bfloat16)
    earlier = (
        lax.broadcasted_iota(jnp.int32, (rows, rows), 0) > lax.broadcasted_iota(jnp.int32, (rows, rows), 1)
    ).astype(jnp.float32).astype(jnp.bfloat16)
    before = jnp.dot(earlier, both, preferred_element_type=jnp.float32)
    chosen = []
    for pick in picks:
        slot = jnp.sum(pick * before, axis=1, keepdims=True)
        chosen.append(jnp.concatenate([pick * (1.0 - slot), pick * slot], axis=1))
    taken = (chosen[0] + chosen[1]).astype(jnp.bfloat16)
    chosen = [c.astype(jnp.bfloat16) for c in chosen]

    there, back = scratch[:8], scratch[8:]
    for p in range(CAP):
        for j in range(chunks // 2):
            placed = lax.dot_general(
                taken[:, p * peers : (p + 1) * peers], normed_ref[:, 2 * j * LANES : (2 * j + 2) * LANES],
                (((0,), (0,)), ((), ())), preferred_element_type=jnp.float32,
            )
            for h in range(2):
                stage[pl.ds(p * chunks + 2 * j + h, peers, stride=span), :] = placed[:, h * LANES : (h + 1) * LANES]
        pack(there, p)
        if p == 0:
            pl.semaphore_wait(barrier, len(ring) + 1)
        begin(there, p)
        if p == 0:
            rest(there, p)
    for p in range(1, CAP):
        rest(there, p)
    for p in range(CAP):
        turn(there, p)
    for load in loads:
        load.wait()

    tile = 256

    def serve(p):
        for l in range(chunks):
            rows_in[:, l * LANES : (l + 1) * LANES] = stage[pl.ds(p * chunks + l, peers, stride=span), :].astype(
                jnp.bfloat16
            )
        hidden = []
        for j in range(wg.shape[1] // tile):
            cols = slice(j * tile, (j + 1) * tile)
            gate = jnp.dot(rows_in[...], wg[:, cols], preferred_element_type=jnp.float32)
            up = jnp.dot(rows_in[...], wu[:, cols], preferred_element_type=jnp.float32)
            hidden.append((gate / (1.0 + jnp.exp(-gate)) * up).astype(jnp.bfloat16))
        hidden = jnp.concatenate(hidden, axis=1)
        for j in range(chunks // 2):
            out = jnp.dot(hidden, wd[:, 2 * j * LANES : (2 * j + 2) * LANES], preferred_element_type=jnp.float32)
            for h in range(2):
                stage[pl.ds(p * chunks + 2 * j + h, peers, stride=span), :] = out[:, h * LANES : (h + 1) * LANES]

    for p in range(CAP):
        finish(there, p)
        unpack(there, p)
        serve(p)
        pack(back, p)
        begin(back, p)
        rest(back, p)
    for p in range(CAP):
        turn(back, p)

    for p in range(CAP):
        finish(back, p)
        unpack(back, p)
        for j in range(chunks // 2):
            block = jnp.concatenate(
                [stage[pl.ds(p * chunks + 2 * j + h, peers, stride=span), :] for h in range(2)], axis=1
            ).astype(jnp.bfloat16)
            cols = slice(2 * j * LANES, (2 * j + 2) * LANES)
            added = 0.0 if p == 0 else sums[:, cols]
            for k in range(TOPK):
                picked = chosen[k][:, p * peers : (p + 1) * peers]
                added = added + mixing[k] * jnp.dot(picked, block, preferred_element_type=jnp.float32)
            if p < CAP - 1:
                sums[:, cols] = added
            else:
                out_ref[:, cols] = (stream_ref[:, cols].astype(jnp.float32) + added).astype(jnp.bfloat16)
    sent(there)
    sent(back)


def routed_experts(sp_n, tp_n, normed, stream, small, w_gate, w_up, w_down):
    rows, width = normed.shape
    peers = sp_n * tp_n
    chips = sp_n // 2
    span = CAP * width // LANES
    vmem = pl.BlockSpec(memory_space=pltpu.VMEM)
    hbm = pl.BlockSpec(memory_space=pl.ANY)
    dma = pltpu.SemaphoreType.DMA

    def blocks(*lead):
        return pltpu.VMEM((*lead, span, LANES), jnp.bfloat16)

    buffers = [
        blocks(2, chips * tp_n), blocks(chips * tp_n), blocks(tp_n, chips), blocks(chips, tp_n), blocks(chips, tp_n),
        blocks(tp_n, chips), dma((CAP, 8)), dma((CAP, 2)),
    ]
    return pl.pallas_call(
        functools.partial(moe_kernel, sp_n, tp_n),
        out_shape=jax.ShapeDtypeStruct((rows, width), jnp.bfloat16),
        in_specs=[vmem] * 3 + [hbm] * 3,
        out_specs=vmem,
        scratch_shapes=[
            pltpu.VMEM(w_gate.shape, jnp.bfloat16),
            pltpu.VMEM(w_up.shape, jnp.bfloat16),
            pltpu.VMEM(w_down.shape, jnp.bfloat16),
            pltpu.VMEM((peers * span, LANES), jnp.float32),
            pltpu.VMEM((peers, width), jnp.bfloat16),
            pltpu.VMEM((rows, width), jnp.float32),
            dma((3,)),
            *buffers,
            *buffers,
        ],
        compiler_params=pltpu.CompilerParams(collective_id=1, has_side_effects=True),
        name="routed_experts",
    )(normed, stream, small, w_gate, w_up, w_down)


def shards(
    residual,
    query,
    latent,
    rope_key,
    latent_gain,
    key_up,
    value_up,
    out_weight,
    norm_gain,
    group_prob,
    pair_logits,
    routes,
    w_gate,
    w_up,
    w_down,
):
    positions_here = query.shape[0]
    own_positions = lax.axis_index("sp") * positions_here + jnp.arange(
        positions_here, dtype=jnp.int32
    )
    row_count = residual.shape[0] * residual.shape[1]
    queries, keyed = prepared(query, latent, rope_key, latent_gain, key_up, value_up, own_positions)
    stream, normed = attention(
        lax.axis_size("sp"),
        lax.axis_size("tp"),
        queries,
        keyed,
        out_weight,
        residual.reshape(row_count, D),
        norm_gain.reshape(1, D),
    )
    small = jnp.concatenate([routes.astype(jnp.float32), pair_logits, group_prob[..., None]], axis=-1)
    combined = routed_experts(
        lax.axis_size("sp"),
        lax.axis_size("tp"),
        normed,
        stream,
        small.reshape(row_count, 2 * TOPK + 1),
        w_gate[0],
        w_up[0],
        w_down[0],
    )
    return combined.reshape(residual.shape)


def solution(mesh):
    placed = (
        P(("sp", "tp"), "grp", None),
        P("sp", "grp", "tp"),
        P("sp", "grp", None),
        P("sp", "grp", None),
        P(),
        P(None, "tp"),
        P(None, "tp"),
        P("tp", None),
        P(),
        P(("sp", "tp"), "grp"),
        P(("sp", "tp"), "grp", None),
        P(("sp", "tp"), "grp", None),
        P(("sp", "tp"), None, None),
        P(("sp", "tp"), None, None),
        P(("sp", "tp"), None, None),
    )
    return jax.shard_map(
        shards, mesh=mesh, in_specs=placed, out_specs=P(("sp", "tp"), "grp", None), check_vma=False
    )
```

```python
import functools
import math

import jax
import jax.numpy as jnp
from jax import lax
from jax.experimental import pallas as pl
from jax.experimental.pallas import tpu as pltpu
from jax.sharding import PartitionSpec as P

D = 2048
NOPE = 128
QK = 192
TOPK = 2
CAP = 2
LANES = 128
MESH = pl.DeviceIdType.MESH


epsilon = 1e-06
rotary_base = 10000.0


def rotate_by(values, positions):
    halfway = values.shape[-1] // 2
    inverse = rotary_base ** (-jnp.arange(halfway, dtype=jnp.float32) / halfway)
    angles = positions.astype(jnp.float32)[:, None] * inverse[None, :]
    cosine_values = jnp.cos(angles)
    sine_values = jnp.sin(angles)
    first_half = values[..., :halfway]
    second_half = values[..., halfway:]
    return jnp.concatenate(
        [
            first_half * cosine_values - second_half * sine_values,
            second_half * cosine_values + first_half * sine_values,
        ],
        axis=-1,
    )


def rms_scale(values, gain_values):
    return (
        values
        * lax.rsqrt(jnp.mean(values * values, axis=-1, keepdims=True) + epsilon)
        * gain_values
    )


def attention_kernel(sp_n, tp_n, seqs, q_ref, kv_ref, ow_ref, res_ref, gain_ref, stream_ref, normed_ref,
                     kv_all, q_all, ow_all, att, heads_y, heads_in, run_max, run_sum, acc,
                     kv_sem, kv_fwd, kv_sib, q_sem, ow_sem, ow_sib, y_sem, x_sem, kv_sent, q_sent, ow_sent, ow_half, ow_sib_sent, y_sent, x_sent):
    chips = sp_n // 2
    side = chips // 2
    half_ring = tp_n // 2
    sp, tp = lax.axis_index("sp"), lax.axis_index("tp")
    chip, core = sp // 2, lax.rem(sp, 2)
    own_seq, own_g = chip // 2, lax.rem(chip, 2)
    half = q_ref.shape[1] // 3
    positions = 2 * half
    part = ow_ref.shape[0] // 2

    def at(chip_id, core_id=None):
        return {"sp": 2 * chip_id + (core if core_id is None else core_id)}

    homes = []
    for e in range(1, seqs):
        seq = lax.rem(own_seq + e, seqs)
        delta = lax.rem(chip - 2 * seq + chips, chips)
        g = 1 - lax.rem(delta + chips - 1, chips) // side
        home = 2 * seq + g
        k = g * lax.rem(chip - home + chips, chips) + (1 - g) * lax.rem(home - chip + chips, chips)
        homes.append((seq, g, home, k))
    sources = [lax.rem(chip + (2 * own_g - 1) * k + chips, chips) for k in range(side)]
    beside = 2 * own_seq + 1 - own_g
    right, left = lax.rem(tp + 1, tp_n), lax.rem(tp + tp_n - 1, tp_n)

    def slot(core_id, g, k):
        return (core_id * 2 + g) * side + k

    def send(src, dst, sent, got, where):
        pltpu.make_async_remote_copy(
            src_ref=src, dst_ref=dst, send_sem=sent, recv_sem=got, device_id=where, device_id_type=MESH
        ).start()

    def landed(buffer, sem):
        pltpu.make_async_copy(buffer, buffer, sem).wait()

    barrier = pltpu.get_barrier_semaphore()
    peers = [at(h[2]) for h in homes] + [at(s) for s in sources[1:]] + [at(beside), at(chip, 1 - core)]
    peers += [{"tp": lax.rem(tp + d, tp_n)} for d in range(1, tp_n)]
    for where in peers:
        pl.semaphore_signal(barrier, inc=1, device_id=where, device_id_type=MESH)
    pl.semaphore_wait(barrier, len(peers))

    own_slot = slot(core, own_g, 0)
    for seq, g, home, k in homes[1:2] + homes[:1] + homes[2:]:
        send(kv_ref.at[seq], kv_all.at[slot(core, g, k)], kv_sent, kv_sem.at[k], at(home))

    def ow_stage(r):
        for way, to in ((0, right), (1, left)):
            head = lax.rem(tp + (r - 1 if way else 1 - r) + tp_n, tp_n)
            if r < half_ring:
                src = ow_ref.at[pl.ds(core * part, part)] if r == 1 else ow_all.at[head, core]
                send(src, ow_all.at[head, core], ow_sent, ow_sem.at[way, r - 1], {"tp": to})
            else:
                rows = pl.ds(way * (part // 2), part // 2)
                src = ow_ref.at[pl.ds(core * part + way * (part // 2), part // 2)] if r == 1 else ow_all.at[head, core, rows]
                send(src, ow_all.at[head, core, rows], ow_half, ow_sem.at[way, r - 1], {"tp": to})

    def ow_arrived(r):
        for way in range(2):
            head = lax.rem(tp + (r if way else -r) + tp_n, tp_n)
            if r < half_ring:
                landed(ow_all.at[head, core], ow_sem.at[way, r - 1])
            else:
                landed(ow_all.at[head, core, pl.ds(way * (part // 2), part // 2)], ow_sem.at[way, r - 1])
            if r < half_ring or way == 1:
                send(ow_all.at[head, core], ow_all.at[head, core], ow_sib_sent, ow_sib, at(chip, 1 - core))
        if r < half_ring:
            ow_stage(r + 1)

    def pass_on(k, src):
        place = kv_all.at[slot(core, own_g, k)]
        send(src, place, kv_sent, kv_fwd.at[k], at(beside))
        send(src, place, kv_sent, kv_sib.at[own_g, k], at(chip, 1 - core))

    pass_on(0, kv_ref.at[own_seq])
    ow_stage(1)
    for seq, g, home, k in homes:
        send(q_ref.at[seq], q_all.at[k], q_sent, q_sem.at[k], at(home))
    kv_all[own_slot] = kv_ref[own_seq]
    q_all[0] = q_ref[own_seq]
    ow_all[tp] = ow_ref[...].reshape(ow_all.shape[1:])

    low = lax.broadcasted_iota(jnp.int32, (half, LANES), 1) < LANES // 2
    factor = QK ** (-0.5) * math.log2(math.e)

    def attend(base, k, first, last):
        def rows(start):
            return kv_all[pl.ds(base, side), start : start + half, :].reshape(side * half, LANES)

        plain = q_all[k, :positions]
        first_rot = q_all[k, positions:].astype(jnp.float32)
        second_rot = pltpu.roll(first_rot, LANES // 2, 1)
        halves = [
            jnp.concatenate([jnp.where(low, first_rot, 0.0), jnp.where(low, second_rot, 0.0)], axis=0),
            jnp.concatenate([jnp.where(low, 0.0, second_rot), jnp.where(low, 0.0, first_rot)], axis=0),
        ]
        turned = rows(4 * half)
        scores = []
        for n in range(2):
            keys = jnp.concatenate([rows(n * half), turned], axis=1)
            q = jnp.concatenate([plain, halves[n].astype(jnp.bfloat16)], axis=1)
            scores.append(
                lax.dot_general(q, keys, (((1,), (1,)), ((), ())), preferred_element_type=jnp.float32)
            )
        top = jnp.maximum(jnp.max(scores[0], axis=1, keepdims=True), jnp.max(scores[1], axis=1, keepdims=True))
        if not first:
            old = run_max[k][:, :1]
            top = jnp.maximum(top, old)
            shrink = jnp.exp2((old - top) * factor)
        total, mixed = 0.0, 0.0
        for n in range(2):
            weights = jnp.exp2((scores[n] - top) * factor)
            total = total + jnp.sum(weights, axis=1, keepdims=True)
            mixed = mixed + jnp.dot(weights.astype(jnp.bfloat16), rows((2 + n) * half), preferred_element_type=jnp.float32)
        if not first:
            total = total + shrink * run_sum[k][:, :1]
            mixed = mixed + shrink * acc[k]
        if last:
            att[k] = (mixed / total).reshape(att.shape[1:]).astype(jnp.bfloat16)
        else:
            run_max[k] = jnp.broadcast_to(top, run_max.shape[1:])
            run_sum[k] = jnp.broadcast_to(total, run_sum.shape[1:])
            acc[k] = mixed

    def attend_all(base, first):
        def body(k, _):
            attend(base, k, first, False)
            return 0

        lax.fori_loop(0, side, body, 0)

    def direct_arrived(k):
        place = kv_all.at[slot(core, own_g, k)]
        landed(place, kv_sem.at[k])
        pass_on(k, place)

    def forward_arrived(k):
        place = kv_all.at[slot(core, 1 - own_g, k)]
        landed(place, kv_fwd.at[k])
        send(place, place, kv_sent, kv_sib.at[1 - own_g, k], at(chip, 1 - core))

    forward_arrived(0)
    for k in range(1, side):
        direct_arrived(k)
        if k == 1:
            ow_arrived(1)
        forward_arrived(k)
    for r in range(2, min(3, half_ring + 1)):
        ow_arrived(r)
    for k in range(1, side):
        landed(q_all.at[k], q_sem.at[k])
    attend_all(slot(core, own_g, 0), True)
    for k in range(side):
        landed(kv_all.at[slot(1 - core, own_g, k)], kv_sib.at[own_g, k])
    attend_all(slot(1 - core, own_g, 0), False)
    for r in range(3, half_ring):
        ow_arrived(r)
    attend_all(slot(core, 1 - own_g, 0), False)
    for k in range(side):
        landed(kv_all.at[slot(1 - core, 1 - own_g, k)], kv_sib.at[1 - own_g, k])
    for k in reversed(range(side)):
        attend(slot(1 - core, 1 - own_g, 0), k, False, True)
        if k > 0:
            send(att.at[k], heads_y.at[own_seq], y_sent, y_sem.at[own_seq], at(sources[k]))
    for e in range(seqs):
        seq, block = own_seq, att.at[0]
        if e > 0:
            seq = homes[e - 1][0]
            block = heads_y.at[seq]
            landed(block, y_sem.at[seq])
        for d in range(1, tp_n):
            to = lax.rem(tp + d, tp_n)
            send(block.at[to], heads_in.at[tp, seq], x_sent, x_sem, {"tp": to})
        heads_in[tp, seq] = block[tp]
    if half_ring > 2:
        ow_arrived(half_ring)
    landed(ow_all.at[pl.ds(0, tp_n - 1), 0], ow_sib)
    landed(heads_in.at[pl.ds(0, tp_n - 1)], x_sem)

    rows, width = res_ref.shape
    each = rows // seqs
    lhs = jnp.concatenate(
        [heads_in[h].astype(jnp.float32).reshape(rows, LANES).astype(jnp.bfloat16) for h in range(tp_n)], axis=1
    )
    r_out = lax.broadcasted_iota(jnp.int32, (rows, rows), 0)
    r_in = lax.broadcasted_iota(jnp.int32, (rows, rows), 1)
    shuffle = (r_in == lax.rem(r_out, seqs) * each + r_out // seqs).astype(jnp.float32).astype(jnp.bfloat16)
    lhs = jnp.dot(shuffle, lhs, preferred_element_type=jnp.float32).astype(jnp.bfloat16)
    squares = 0.0
    tile = 2 * LANES
    for j in range(width // tile):
        cols = slice(j * tile, (j + 1) * tile)
        weight = ow_all[:, :, :, cols].reshape(lhs.shape[1], tile)
        summed = res_ref[:, cols].astype(jnp.float32) + jnp.dot(lhs, weight, preferred_element_type=jnp.float32)
        rounded = summed.astype(jnp.bfloat16)
        stream_ref[:, cols] = rounded
        wide = rounded.astype(jnp.float32)
        squares = squares + jnp.sum(wide * wide, axis=1, keepdims=True)
    scale = lax.rsqrt(squares / width + epsilon)
    for j in range(width // tile):
        cols = slice(j * tile, (j + 1) * tile)
        normed_ref[:, cols] = (stream_ref[:, cols].astype(jnp.float32) * scale * gain_ref[:, cols]).astype(jnp.bfloat16)

    landed(kv_all.at[pl.ds(0, 4 * side - 1)], kv_sent)
    if seqs > 1:
        landed(q_all.at[pl.ds(0, seqs - 1)], q_sent)
        landed(att.at[pl.ds(0, side - 1)], y_sent)
    if half_ring > 1:
        landed(ow_all.at[pl.ds(0, 2 * (half_ring - 1)), 0], ow_sent)
    landed(ow_all.at[0, 0], ow_half)
    landed(ow_all.at[pl.ds(0, tp_n - 1), 0], ow_sib_sent)
    landed(heads_in.at[pl.ds(0, tp_n - 1)], x_sent)


def attention(sp_n, tp_n, queries, keyed, out_weight, residual, norm_gain):
    seqs, positions = queries.shape[0], queries.shape[1] // 3 * 2
    rows, width = residual.shape
    side = sp_n // 4
    each = positions // tp_n
    vmem = pl.BlockSpec(memory_space=pltpu.VMEM)
    dma = pltpu.SemaphoreType.DMA
    bf16, f32 = jnp.bfloat16, jnp.float32
    return pl.pallas_call(
        functools.partial(attention_kernel, sp_n, tp_n, seqs),
        out_shape=[jax.ShapeDtypeStruct((rows, width), bf16)] * 2,
        in_specs=[vmem] * 5,
        out_specs=[vmem] * 2,
        scratch_shapes=[
            pltpu.VMEM((4 * side,) + keyed.shape[1:], bf16),
            pltpu.VMEM((side,) + queries.shape[1:], bf16),
            pltpu.VMEM((tp_n, 2, out_weight.shape[0] // 2, width), bf16),
            pltpu.VMEM((side, tp_n, each, LANES), bf16),
            pltpu.VMEM((seqs, tp_n, each, LANES), bf16),
            pltpu.VMEM((tp_n, seqs, each, LANES), bf16),
            pltpu.VMEM((side, positions, LANES), f32),
            pltpu.VMEM((side, positions, LANES), f32),
            pltpu.VMEM((side, positions, LANES), f32),
            dma((side,)), dma((side,)), dma((2, side)), dma((side,)), dma((2, tp_n // 2)),
            dma, dma((seqs,)), dma, dma, dma, dma, dma, dma, dma, dma,
        ],
        compiler_params=pltpu.CompilerParams(collective_id=2, has_side_effects=True),
        name="attention",
    )(queries, keyed, out_weight, residual, norm_gain)


def prepared(query, latent, rope_key, latent_gain, key_up, value_up, own_positions):
    seqs = query.shape[1]
    half = query.shape[0] // 2
    by_seq = query.transpose(1, 0, 2)
    turned = rotate_by(by_seq[..., NOPE:].astype(jnp.float32), own_positions).astype(jnp.bfloat16)
    turned = jnp.concatenate([turned[:, :half], turned[:, half:]], axis=-1)
    queries = jnp.concatenate([by_seq[..., :NOPE], turned], axis=1)
    rows = latent.transpose(1, 0, 2)
    normed = rms_scale(rows.astype(jnp.float32), latent_gain).astype(jnp.bfloat16)
    keys = jnp.dot(normed, key_up, preferred_element_type=jnp.float32).astype(jnp.bfloat16)
    values = jnp.dot(normed, value_up, preferred_element_type=jnp.float32).astype(jnp.bfloat16)
    key_rot = rotate_by(rope_key.transpose(1, 0, 2).astype(jnp.float32), own_positions).astype(jnp.bfloat16)
    packed = jnp.concatenate([key_rot[:, :half], key_rot[:, half:]], axis=-1)
    return queries, jnp.concatenate([keys, values, packed], axis=1)


def moe_kernel(sp_n, tp_n, normed_ref, stream_ref, small_ref, wg_hbm, wu_hbm, wd_hbm, out_ref,
               wg, wu, wd, stage, rows_in, sums, w_sems, *scratch):
    chips = sp_n // 2
    peers = sp_n * tp_n
    plane = chips * tp_n
    rows, width = normed_ref.shape
    chunks = width // LANES
    span = CAP * chunks
    sp, tp = lax.axis_index("sp"), lax.axis_index("tp")
    chip, core = sp // 2, lax.rem(sp, 2)
    barrier = pltpu.get_barrier_semaphore()
    sibling = {"sp": 2 * chip + 1 - core}

    def across(d):
        to = lax.rem(tp + d, tp_n)
        return to, {"tp": to}

    def along(d):
        to = lax.rem(chip + d, chips)
        return to, {"sp": 2 * to + core}

    ring = []
    for d in reversed(range(1, max(chips, tp_n) // 2 + 1)):
        for step in (d, -d):
            if d < tp_n and (step > 0 or 2 * d != tp_n) and d <= tp_n // 2:
                ring.append((across, step % tp_n))
            if d < chips and (step > 0 or 2 * d != chips) and d <= chips // 2:
                ring.append((along, step % chips))
    for where in [sibling] + [way(d)[1] for way, d in ring]:
        pl.semaphore_signal(barrier, inc=1, device_id=where, device_id_type=MESH)
    loads = [
        pltpu.make_async_copy(src, dst, w_sems.at[k])
        for k, (src, dst) in enumerate(((wg_hbm, wg), (wu_hbm, wu), (wd_hbm, wd)))
    ]
    for load in loads:
        load.start()

    def send(src, dst, sent, got, where):
        pltpu.make_async_remote_copy(
            src_ref=src, dst_ref=dst, send_sem=sent, recv_sem=got, device_id=where, device_id_type=MESH
        ).start()

    def landed(buffer, sem):
        pltpu.make_async_copy(buffer, buffer, sem).wait()

    def part(p):
        return pl.ds(p * chunks, chunks)

    def begin(buffers, p):
        held, given, by_tp, by_sp, from_even, from_odd, sems, swap = buffers
        send(given.at[:, part(p)], held.at[core, :, part(p)], swap.at[p, 0], swap.at[p, 1], sibling)
        pl.when(core == 0)(functools.partial(even_first, buffers, p))
        pl.when(core == 1)(functools.partial(odd_first, buffers, p))

    def even_first(buffers, p):
        held, given, by_tp, by_sp, from_even, from_odd, sems, swap = buffers
        for way, d in ring:
            if way is across:
                to, where = across(d)
                src = held.at[0, pl.ds(to * chips, chips), part(p)]
                send(src, by_tp.at[tp, :, part(p)], sems.at[p, 0], sems.at[p, 1], where)

    def odd_first(buffers, p):
        held, given, by_tp, by_sp, from_even, from_odd, sems, swap = buffers
        for way, d in ring:
            if way is along:
                to, where = along(d)
                src = held.at[1, pl.ds(to * tp_n, tp_n), part(p)]
                send(src, by_sp.at[chip, :, part(p)], sems.at[p, 2], sems.at[p, 3], where)

    def rest(buffers, p):
        held, given, by_tp, by_sp, from_even, from_odd, sems, swap = buffers
        landed(given.at[:, part(p)], swap.at[p, 1])
        pl.when(core == 1)(functools.partial(even_first, buffers, p))
        pl.when(core == 0)(functools.partial(odd_first, buffers, p))
        by_tp[tp, :, part(p)] = held[0, pl.ds(tp * chips, chips), part(p)]
        by_sp[chip, :, part(p)] = held[1, pl.ds(chip * tp_n, tp_n), part(p)]

    def turn(buffers, p):
        held, given, by_tp, by_sp, from_even, from_odd, sems, swap = buffers
        landed(by_tp.at[pl.ds(0, tp_n - 1), :, part(p)], sems.at[p, 1])
        for way, d in ring:
            if way is along:
                to, where = along(d)
                send(by_tp.at[:, to, part(p)], from_even.at[chip, :, part(p)], sems.at[p, 4], sems.at[p, 5], where)
        landed(by_sp.at[pl.ds(0, chips - 1), :, part(p)], sems.at[p, 3])
        for way, d in ring:
            if way is across:
                to, where = across(d)
                send(by_sp.at[:, to, part(p)], from_odd.at[tp, :, part(p)], sems.at[p, 6], sems.at[p, 7], where)
        from_even[chip, :, part(p)] = by_tp[:, chip, part(p)]
        from_odd[tp, :, part(p)] = by_sp[:, tp, part(p)]

    def finish(buffers, p):
        held, given, by_tp, by_sp, from_even, from_odd, sems, swap = buffers
        landed(from_even.at[pl.ds(0, chips - 1), :, part(p)], sems.at[p, 5])
        landed(from_odd.at[pl.ds(0, tp_n - 1), :, part(p)], sems.at[p, 7])

    def sent(buffers):
        held, given, by_tp, by_sp, from_even, from_odd, sems, swap = buffers
        for p in range(CAP):
            landed(given.at[:, part(p)], swap.at[p, 0])
            landed(by_tp.at[pl.ds(0, tp_n - 1), :, part(p)], sems.at[p, 0])
            landed(by_sp.at[pl.ds(0, chips - 1), :, part(p)], sems.at[p, 2])
            landed(from_even.at[pl.ds(0, chips - 1), :, part(p)], sems.at[p, 4])
            landed(from_odd.at[pl.ds(0, tp_n - 1), :, part(p)], sems.at[p, 6])

    def device(c, core_id, x):
        return (2 * c + core_id) * tp_n + x

    step = min(8, plane)

    def pack(buffers, p):
        held, given = buffers[:2]

        def block(i, to_core):
            c = lax.rem(i, chips) * (1 - core) + i // tp_n * core
            x = i // chips * (1 - core) + lax.rem(i, tp_n) * core
            start = pl.multiple_of(device(c, to_core, x) * span, span) + p * chunks
            return stage[pl.ds(start, chunks), :].astype(jnp.bfloat16)

        def body(n, _):
            for j in range(step):
                i = n * step + j
                held[core, i, part(p)] = block(i, core)
                given[i, part(p)] = block(i, 1 - core)
            return 0

        lax.fori_loop(0, plane // step, body, 0)

    def unpack(buffers, p):
        from_even, from_odd = buffers[4:6]

        def put(where, block):
            start = pl.multiple_of(where * span, span) + p * chunks
            stage[pl.ds(start, chunks), :] = block.astype(jnp.float32)

        def body(n, _):
            for j in range(step):
                i = n * step + j
                c, x = i // tp_n, lax.rem(i, tp_n)
                put(device(c, 0, x), from_even[c, x, part(p)])
                put(device(c, 1, x), from_odd[x, c, part(p)])
            return 0

        lax.fori_loop(0, plane // step, body, 0)

    experts = lax.broadcasted_iota(jnp.int32, (rows, peers), 1).astype(jnp.float32)
    small = small_ref[...]
    picks = [(small[:, k : k + 1] == experts).astype(jnp.float32) for k in range(TOPK)]
    logits = [small[:, TOPK + k : TOPK + k + 1] for k in range(TOPK)]
    top = jnp.maximum(logits[0], logits[1])
    raised = [jnp.exp(v - top) for v in logits]
    shared = small[:, 2 * TOPK : 2 * TOPK + 1]
    mixing = [v / (raised[0] + raised[1]) * shared for v in raised]
    both = (picks[0] + picks[1]).astype(jnp.bfloat16)
    earlier = (
        lax.broadcasted_iota(jnp.int32, (rows, rows), 0) > lax.broadcasted_iota(jnp.int32, (rows, rows), 1)
    ).astype(jnp.float32).astype(jnp.bfloat16)
    before = jnp.dot(earlier, both, preferred_element_type=jnp.float32)
    chosen = []
    for pick in picks:
        slot = jnp.sum(pick * before, axis=1, keepdims=True)
        chosen.append(jnp.concatenate([pick * (1.0 - slot), pick * slot], axis=1))
    taken = (chosen[0] + chosen[1]).astype(jnp.bfloat16)
    chosen = [c.astype(jnp.bfloat16) for c in chosen]

    there, back = scratch[:8], scratch[8:]
    for p in range(CAP):
        for j in range(chunks // 2):
            placed = lax.dot_general(
                taken[:, p * peers : (p + 1) * peers], normed_ref[:, 2 * j * LANES : (2 * j + 2) * LANES],
                (((0,), (0,)), ((), ())), preferred_element_type=jnp.float32,
            )
            for h in range(2):
                stage[pl.ds(p * chunks + 2 * j + h, peers, stride=span), :] = placed[:, h * LANES : (h + 1) * LANES]
        pack(there, p)
        if p == 0:
            pl.semaphore_wait(barrier, len(ring) + 1)
        begin(there, p)
        if p == 0:
            rest(there, p)
    for p in range(1, CAP):
        rest(there, p)
    for p in range(CAP):
        turn(there, p)
    for load in loads:
        load.wait()

    tile = 256

    def serve(p):
        for l in range(chunks):
            rows_in[:, l * LANES : (l + 1) * LANES] = stage[pl.ds(p * chunks + l, peers, stride=span), :].astype(
                jnp.bfloat16
            )
        hidden = []
        for j in range(wg.shape[1] // tile):
            cols = slice(j * tile, (j + 1) * tile)
            gate = jnp.dot(rows_in[...], wg[:, cols], preferred_element_type=jnp.float32)
            up = jnp.dot(rows_in[...], wu[:, cols], preferred_element_type=jnp.float32)
            hidden.append((gate / (1.0 + jnp.exp(-gate)) * up).astype(jnp.bfloat16))
        hidden = jnp.concatenate(hidden, axis=1)
        for j in range(chunks // 2):
            out = jnp.dot(hidden, wd[:, 2 * j * LANES : (2 * j + 2) * LANES], preferred_element_type=jnp.float32)
            for h in range(2):
                stage[pl.ds(p * chunks + 2 * j + h, peers, stride=span), :] = out[:, h * LANES : (h + 1) * LANES]

    for p in range(CAP):
        finish(there, p)
        unpack(there, p)
        serve(p)
        pack(back, p)
        begin(back, p)
        rest(back, p)
    for p in range(CAP):
        turn(back, p)

    for p in range(CAP):
        finish(back, p)
        unpack(back, p)
        for j in range(chunks // 2):
            block = jnp.concatenate(
                [stage[pl.ds(p * chunks + 2 * j + h, peers, stride=span), :] for h in range(2)], axis=1
            ).astype(jnp.bfloat16)
            cols = slice(2 * j * LANES, (2 * j + 2) * LANES)
            added = 0.0 if p == 0 else sums[:, cols]
            for k in range(TOPK):
                picked = chosen[k][:, p * peers : (p + 1) * peers]
                added = added + mixing[k] * jnp.dot(picked, block, preferred_element_type=jnp.float32)
            if p < CAP - 1:
                sums[:, cols] = added
            else:
                summed = stream_ref[:, cols].astype(jnp.float32) + added
                out_ref[:, :, cols] = summed.reshape(*out_ref.shape[:2], 2 * LANES).astype(jnp.bfloat16)
    sent(there)
    sent(back)


def routed_experts(sp_n, tp_n, shape, normed, stream, small, w_gate, w_up, w_down):
    rows, width = normed.shape
    peers = sp_n * tp_n
    chips = sp_n // 2
    span = CAP * width // LANES
    vmem = pl.BlockSpec(memory_space=pltpu.VMEM)
    hbm = pl.BlockSpec(memory_space=pl.ANY)
    dma = pltpu.SemaphoreType.DMA

    def blocks(*lead):
        return pltpu.VMEM((*lead, span, LANES), jnp.bfloat16)

    buffers = [
        blocks(2, chips * tp_n), blocks(chips * tp_n), blocks(tp_n, chips), blocks(chips, tp_n), blocks(chips, tp_n),
        blocks(tp_n, chips), dma((CAP, 8)), dma((CAP, 2)),
    ]
    return pl.pallas_call(
        functools.partial(moe_kernel, sp_n, tp_n),
        out_shape=jax.ShapeDtypeStruct(shape, jnp.bfloat16),
        in_specs=[vmem] * 3 + [hbm] * 3,
        out_specs=vmem,
        scratch_shapes=[
            pltpu.VMEM(w_gate.shape, jnp.bfloat16),
            pltpu.VMEM(w_up.shape, jnp.bfloat16),
            pltpu.VMEM(w_down.shape, jnp.bfloat16),
            pltpu.VMEM((peers * span, LANES), jnp.float32),
            pltpu.VMEM((peers, width), jnp.bfloat16),
            pltpu.VMEM((rows, width), jnp.float32),
            dma((3,)),
            *buffers,
            *buffers,
        ],
        compiler_params=pltpu.CompilerParams(collective_id=1, has_side_effects=True),
        name="routed_experts",
    )(normed, stream, small, w_gate, w_up, w_down)


def shards(
    residual,
    query,
    latent,
    rope_key,
    latent_gain,
    key_up,
    value_up,
    out_weight,
    norm_gain,
    group_prob,
    pair_logits,
    routes,
    w_gate,
    w_up,
    w_down,
):
    positions_here = query.shape[0]
    own_positions = lax.axis_index("sp") * positions_here + jnp.arange(
        positions_here, dtype=jnp.int32
    )
    row_count = residual.shape[0] * residual.shape[1]
    queries, keyed = prepared(query, latent, rope_key, latent_gain, key_up, value_up, own_positions)
    stream, normed = attention(
        lax.axis_size("sp"),
        lax.axis_size("tp"),
        queries,
        keyed,
        out_weight,
        residual.reshape(row_count, D),
        norm_gain.reshape(1, D),
    )
    small = jnp.concatenate([routes.astype(jnp.float32), pair_logits, group_prob[..., None]], axis=-1)
    return routed_experts(
        lax.axis_size("sp"),
        lax.axis_size("tp"),
        residual.shape,
        normed,
        stream,
        small.reshape(row_count, 2 * TOPK + 1),
        w_gate[0],
        w_up[0],
        w_down[0],
    )


def solution(mesh):
    placed = (
        P(("sp", "tp"), "grp", None),
        P("sp", "grp", "tp"),
        P("sp", "grp", None),
        P("sp", "grp", None),
        P(),
        P(None, "tp"),
        P(None, "tp"),
        P("tp", None),
        P(),
        P(("sp", "tp"), "grp"),
        P(("sp", "tp"), "grp", None),
        P(("sp", "tp"), "grp", None),
        P(("sp", "tp"), None, None),
        P(("sp", "tp"), None, None),
        P(("sp", "tp"), None, None),
    )
    return jax.shard_map(
        shards, mesh=mesh, in_specs=placed, out_specs=P(("sp", "tp"), "grp", None), check_vma=False
    )
```
